256 devices in a mesh: fs: 32 (over z, y), tp: 8 (over x, core).
Axes of the slice: x: 4, y: 4, z: 8, core: 2. Of those that a mesh axis runs over, the one named last changes fastest.
Arguments:
- latent_in: bfloat16 [98304, 512], P('fs'), may hold values from -6 to 6
- query_cot: bfloat16 [98304, 1536], P('fs', 'tp'), may hold values from -6 to 6
- attn_out: bfloat16 [98304, 1024], P('fs'), may hold values from -6 to 6
- mix_cot: bfloat16 [98304, 2048], P('fs', 'tp'), may hold values from -6 to 6
- query_weight: float32 [512, 1536], P('fs', 'tp'), may hold values from -0.25 to 0.25
- output_weight: float32 [1024, 2048], P('fs', 'tp'), may hold values from -0.1875 to 0.1875
- query_factor: bfloat16 [512, 256], P('fs'), may hold values from -0.25 to 0.25
- output_factor: bfloat16 [1024, 256], P('fs'), may hold values from -0.1875 to 0.1875
- query_mean: float32 [256, 1536], P('fs', 'tp'), may hold values from -3 to 3
- query_square: float32 [256, 1536], P('fs', 'tp'), may hold values from 0.05 to 1
- output_mean: float32 [256, 2048], P('fs', 'tp'), may hold values from -3 to 3
- output_square: float32 [256, 2048], P('fs', 'tp'), may hold values from 0.05 to 1
Outputs:
- step_query: float32 [512, 1536], P('fs', 'tp')
- step_output: float32 [1024, 2048], P('fs', 'tp')
- new_query: float32 [512, 1536], P('fs', 'tp')
- new_output: float32 [1024, 2048], P('fs', 'tp')
- copy_query: bfloat16 [512, 1536], P(None, 'tp')
- copy_output: bfloat16 [1024, 2048], P(None, 'tp')
- query_mean_new: float32 [256, 1536], P('fs', 'tp')
- query_square_new: float32 [256, 1536], P('fs', 'tp')
- output_mean_new: float32 [256, 2048], P('fs', 'tp')
- output_square_new: float32 [256, 2048], P('fs', 'tp')
The draws below stay inside these ranges and needn't reach their ends.
All inputs are finite; a program needn't handle non-finite values.
Results may differ from the reference program's by a relative error of at most 0.0085.
Values may be sent and summed in bfloat16 or wider, within the bound.
A program may use at most 64 MiB of HBM per device.

```python
import math
import jax
import jax.numpy as jnp
from jax import lax

D = 2048
Q_RANK = 512
RANK = 256
QCOLS = 1536
HV = 1024
TOKENS = 98304


def level_of(key, extent, cuts, smallest, top_value):
    loudness, own = 1.0, jax.random.fold_in(key, 6)
    for axis_at, blocks in cuts:
        draws = jnp.exp(jax.random.uniform(jax.random.fold_in(own, axis_at), (blocks,), jnp.float32, smallest / len(cuts), top_value / len(cuts)))
        loudness = loudness * jnp.repeat(draws, extent[axis_at] // blocks).reshape([-1 if axis == axis_at else 1 for axis in range(len(extent))])
    return loudness


def normal_values(rng, extent, width, limit, shards=(), held_as=jnp.bfloat16):
    factor_of = level_of(rng, extent, shards, -0.22, 0.18) if shards else 1.0
    values = jax.random.normal(rng, extent, jnp.float32) * width * factor_of
    return jnp.minimum(jnp.maximum(values, -limit), limit).astype(held_as)


def setup_inputs(seed: int = 0) -> dict:
    key_of = jax.random.split(jax.random.key(seed), 13)
    latent_in = normal_values(key_of[0], (TOKENS, Q_RANK), 1.0, 6.0, ((0, 32),))
    query_cot = normal_values(key_of[1], (TOKENS, QCOLS), 1.0, 6.0, ((0, 32), (1, 8)))
    attn_out = normal_values(key_of[2], (TOKENS, HV), 1.0, 6.0, ((0, 32),))
    mix_cot = normal_values(key_of[3], (TOKENS, D), 1.0, 6.0, ((0, 32), (1, 8)))
    query_weight = normal_values(key_of[4], (Q_RANK, QCOLS), Q_RANK ** -0.5, 0.25, ((0, 32), (1, 8)), jnp.float32)
    output_weight = normal_values(key_of[5], (HV, D), HV ** -0.5, 0.1875, ((0, 32), (1, 8)), jnp.float32)
    query_factor = normal_values(key_of[6], (Q_RANK, RANK), Q_RANK ** -0.5, 0.25, ((0, 32),))
    output_factor = normal_values(key_of[7], (HV, RANK), HV ** -0.5, 0.1875, ((0, 32),))
    query_mean = normal_values(key_of[8], (RANK, QCOLS), 0.5, 3.0, ((0, 32), (1, 8)), jnp.float32)
    query_square = jnp.clip(jnp.exp(math.log(1.0) - 2.9957323 * jax.random.uniform(key_of[9], (RANK, QCOLS), jnp.float32) ** level_of(key_of[9], (RANK, QCOLS), ((0, 32), (1, 8)), -0.2, 0.2)), 0.05, 1.0)
    output_mean = normal_values(key_of[10], (RANK, D), 0.5, 3.0, ((0, 32), (1, 8)), jnp.float32)
    output_square = jnp.clip(jnp.exp(math.log(1.0) - 2.9957323 * jax.random.uniform(key_of[11], (RANK, D), jnp.float32) ** level_of(key_of[11], (RANK, D), ((0, 32), (1, 8)), -0.2, 0.2)), 0.05, 1.0)
    return {"latent_in": latent_in, "query_cot": query_cot, "attn_out": attn_out, "mix_cot": mix_cot, "query_weight": query_weight, "output_weight": output_weight, "query_factor": query_factor, "output_factor": output_factor, "query_mean": query_mean, "query_square": query_square, "output_mean": output_mean, "output_square": output_square}


def over_rows(left, right):
    return lax.dot_general(left, right, (((0,), (0,)), ((), ())), preferred_element_type=jnp.float32)

def exact_dot(left, right):
    return jnp.dot(left, right, precision=lax.Precision.HIGHEST, preferred_element_type=jnp.float32)

def moments(mean, square, low):
    mean_new = 0.8 * mean + 0.2 * low
    square_new = 0.9 * square + 0.1 * low * low
    return (mean_new, square_new, mean_new / jnp.sqrt(square_new))

def reference(latent_in, query_cot, attn_out, mix_cot, query_weight, output_weight, query_factor, output_factor, query_mean, query_square, output_mean, output_square):
    inv_root = 1.0 / math.sqrt(latent_in.shape[0])
    grad_query = over_rows(latent_in, query_cot) * inv_root
    grad_output = over_rows(attn_out, mix_cot) * inv_root
    factor_query = query_factor.astype(jnp.float32)
    factor_output = output_factor.astype(jnp.float32)
    low_query = exact_dot(factor_query.T, grad_query)
    low_output = exact_dot(factor_output.T, grad_output)
    mean_q, square_q, direction_q = moments(query_mean, query_square, low_query)
    mean_o, square_o, direction_o = moments(output_mean, output_square, low_output)
    scale_q = 1.0 / jnp.sqrt(jnp.mean(direction_q * direction_q) + 0.25)
    scale_o = 1.0 / jnp.sqrt(jnp.mean(direction_o * direction_o) + 0.25)
    step_q = exact_dot(factor_query, direction_q) * scale_q
    step_o = exact_dot(factor_output, direction_o) * scale_o
    new_q = query_weight - 0.02 * step_q
    new_o = output_weight - 0.02 * step_o
    return (step_q, step_o, new_q, new_o, new_q.astype(jnp.bfloat16), new_o.astype(jnp.bfloat16), mean_q, square_q, mean_o, square_o)
```

```python
import functools
import math

import jax
import jax.numpy as jnp
from jax import lax
from jax.experimental import pallas as pl
from jax.experimental.pallas import tpu as pltpu
from jax.sharding import PartitionSpec as P

MESH = pl.DeviceIdType.MESH
F32 = jnp.float32
BF16 = jnp.bfloat16
NZ, NY = 8, 4
CHUNKS = 6
Z_ORDER = (1, 7, 2, 6, 3, 5, 4)
FAR_FIRST = (4, 3, 5, 2, 6, 1, 7)
FORWARD_UP = (0, 7, 6, 5)
FORWARD_DOWN = (1, 2, 3, 4)


def by_tokens(left, right):
    return lax.dot_general(left, right, (((0,), (0,)), ((), ())), preferred_element_type=F32)


def dot(left, right):
    return jnp.dot(left, right, preferred_element_type=F32)


def split_dot(left, right):
    high = left.astype(BF16)
    low = (left - high.astype(F32)).astype(BF16)
    return dot(high, right) + dot(low, right)


def kernel(
    inv_root,
    lat, qcot, att, mix, qw, ow, qf, of, qm, qs, om, os_,
    step_q, step_o, new_q, new_o, copy_q, copy_o, mean_q, square_q, mean_o, square_o,
    lat_v, qcot_v, att_v, mix_v, qw_v, ow_v, qm_v, qs_v, om_v, os_v,
    gq, go, fac, wei, part, part_in, mid, mid_in, drc, sums, sums_in,
    pq, po, cq, co, sq_v, so_v, nq_v, no_v, mq_v, sqq_v, mo_v, soo_v,
    chunk_sem, small_sem, out_sem,
    fz_s, fz_r, fy_s, fy_r, fw_s, fw_r, fd_s, fd_r,
    wz_s, wz_r, wy_s, wy_r, ww_s, ww_r,
    py_s, py_r, pz_s, pz_r,
    dz_s, dz_r, dy_s, dy_r, dw_s, dw_r,
    st_s, st_r, sy_s, sy_r,
):
    fs, tp = lax.axis_index("fs"), lax.axis_index("tp")
    y, z = lax.rem(fs, NY), fs // NY
    core = lax.rem(tp, 2)
    other = 1 - core
    partner = (fs, tp + 1 - 2 * core)
    ups = [lax.rem(y + d, NY) for d in range(NY)]
    downs = [lax.rem(y + NY - d, NY) for d in range(NY)]
    zup = [lax.rem(z + d, NZ) for d in range(NZ)]
    zdn = [lax.rem(z + NZ - d, NZ) for d in range(NZ)]

    def at_y(row):
        return (z * NY + row, tp)

    def at_z(level):
        return (level * NY + y, tp)

    def at_tp(d):
        return (fs, lax.rem(tp + d, 8))

    def remote(src, dst, send, recv, to):
        return pltpu.make_async_remote_copy(
            src_ref=src, dst_ref=dst, send_sem=send, recv_sem=recv, device_id=to, device_id_type=MESH
        )

    barrier = pltpu.get_barrier_semaphore()
    for to in [at_y(ups[d]) for d in range(1, NY)] + [at_z(zup[d]) for d in range(1, NZ)] + [at_tp(d) for d in range(1, 8)]:
        pl.semaphore_signal(barrier, inc=1, device_id=to, device_id_type=MESH)

    half = pl.ds(pl.multiple_of(core * 128, 128), 128)
    own = fac.at[core, z, y]
    small = []
    for i, (src, dst) in enumerate((
        (qf.at[:, half], own.at[pl.ds(0, 16)]),
        (of.at[:, half], own.at[pl.ds(16, 32)]),
        (qw, qw_v), (ow, ow_v), (qm, qm_v), (qs, qs_v), (om, om_v), (os_, os_v),
    )):
        small.append(pltpu.make_async_copy(src, dst, small_sem.at[i]))
        small[-1].start()

    tokens = lat.shape[0]
    rows = tokens // CHUNKS
    pairs = ((qcot, qcot_v), (lat, lat_v), (mix, mix_v), (att, att_v))

    def chunk_copies(i):
        span = pl.ds(pl.multiple_of(i * rows, rows), rows)
        return [
            pltpu.make_async_copy(src.at[span], dst.at[span], chunk_sem.at[i, j])
            for j, (src, dst) in enumerate(pairs)
        ]

    for i in range(CHUNKS):
        for copy in chunk_copies(i):
            copy.start()

    gq[...] = jnp.zeros_like(gq)
    go[...] = jnp.zeros_like(go)

    def add_chunk(i):
        for copy in chunk_copies(i):
            copy.wait()
        span = pl.ds(pl.multiple_of(i * rows, rows), rows)
        gq[...] += by_tokens(qcot_v[span, :], lat_v[span, :])
        go[...] += by_tokens(mix_v[span, :], att_v[span, :])

    def add_chunks(a, b):
        @pl.loop(a, b)
        def _(i):
            add_chunk(i)

    for copy in small:
        copy.wait()
    qcols = qw_v.shape[1]
    wei[z, y, 0:16, 0:qcols] = qw_v[...].astype(BF16)
    wei[z, y, 16:48, :] = ow_v[...].astype(BF16)

    add_chunks(0, 1)
    pl.semaphore_wait(barrier, 17)

    def f_blk(level, row):
        return fac.at[core, level, row]

    def w_blk(level, row):
        return wei.at[level, row]

    def d_blk(level, row):
        return drc.at[level, row]

    started = []

    def start(copy):
        copy.start()
        started.append(copy)

    def z_send(blk, s, r):
        for k in FAR_FIRST:
            start(remote(blk(z, y), blk(z, y), s.at[k], r.at[k], at_z(zup[k])))

    def z_wait(blk, s, r, k):
        remote(blk(zdn[k], y), blk(zdn[k], y), s.at[k], r.at[k], at_z(zup[k])).wait_recv()

    def y_send(blk, s, r, k):
        for way, row in ((0, ups[1]), (1, downs[1])):
            start(remote(blk(zdn[k], y), blk(zdn[k], y), s.at[way, k], r.at[way, k], at_y(row)))

    def y_wait(blk, s, r, way, k):
        row = downs[1] if way == 0 else ups[1]
        remote(blk(zdn[k], row), blk(zdn[k], row), s.at[way, k], r.at[way, k], at_y(row)).wait_recv()

    def w_send(blk, s, r, k):
        if k in FORWARD_UP:
            src, to = blk(zdn[k], downs[1]), ups[1]
        else:
            src, to = blk(zdn[k], ups[1]), downs[1]
        start(remote(src, src, s.at[k], r.at[k], at_y(to)))

    def w_wait(blk, s, r, k):
        dst = blk(zdn[k], ups[2])
        remote(dst, dst, s.at[k], r.at[k], at_y(ups[1])).wait_recv()

    def swap_send(row, i):
        src = fac.at[core, :, row]
        start(remote(src, src, fd_s.at[i], fd_r.at[i], partner))

    def swap_wait(row, i):
        dst = fac.at[other, :, row]
        remote(dst, dst, fd_s.at[i], fd_r.at[i], partner).wait_recv()

    z_send(f_blk, fz_s, fz_r)
    y_send(f_blk, fy_s, fy_r, 0)
    z_send(w_blk, wz_s, wz_r)
    add_chunks(1, 3)
    for k in Z_ORDER[:4]:
        z_wait(f_blk, fz_s, fz_r, k)
        y_send(f_blk, fy_s, fy_r, k)
    add_chunks(3, 4)
    for k in Z_ORDER[4:]:
        z_wait(f_blk, fz_s, fz_r, k)
        y_send(f_blk, fy_s, fy_r, k)
    swap_send(y, 0)
    order = (0,) + Z_ORDER
    for k in order[:4]:
        for way in (0, 1):
            y_wait(f_blk, fy_s, fy_r, way, k)
        w_send(f_blk, fw_s, fw_r, k)
    add_chunks(4, CHUNKS)
    for k in order[4:]:
        for way in (0, 1):
            y_wait(f_blk, fy_s, fy_r, way, k)
        w_send(f_blk, fw_s, fw_r, k)
    swap_send(downs[1], 1)
    swap_send(ups[1], 2)
    for k in order:
        w_wait(f_blk, fw_s, fw_r, k)
    swap_send(ups[2], 3)
    for i, row in enumerate((y, ups[1], downs[1], ups[2])):
        swap_wait(row, i)

    def factor(first, count):
        return jnp.concatenate(
            [fac[c, :, :, first:first + count, :].reshape(32 * count, 128) for c in (0, 1)], axis=1
        )

    low_q = split_dot(gq[...], factor(0, 16)) * inv_root
    low_q = jnp.concatenate([low_q, jnp.zeros((256 - qcols, 256), F32)], axis=0).T
    low_o = (split_dot(go[...], factor(16, 32)) * inv_root).T
    for row in range(NY):
        part[row] = jnp.concatenate(
            [low_q.reshape(NZ, NY, 8, 256)[:, row], low_o.reshape(NZ, NY, 8, 256)[:, row]], axis=1
        ).astype(BF16)

    for d in (2, 1, 3):
        start(remote(part.at[ups[d]], part_in.at[d], py_s.at[d], py_r.at[d], at_y(ups[d])))
    for k in Z_ORDER:
        z_wait(w_blk, wz_s, wz_r, k)
    for way, row in ((0, ups[1]), (1, downs[1])):
        src = wei.at[:, y]
        start(remote(src, src, wy_s.at[way], wy_r.at[way], at_y(row)))
    total = part[y].astype(F32)
    for d in (1, 3, 2):
        remote(part.at[y], part_in.at[d], py_s.at[d], py_r.at[d], at_y(ups[d])).wait_recv()
        total = total + part_in[d].astype(F32)
    mid[...] = total.astype(BF16)
    for k in FAR_FIRST:
        start(remote(mid.at[zup[k]], mid_in.at[k], pz_s.at[k], pz_r.at[k], at_z(zup[k])))
    low = mid[z].astype(F32)
    for k in Z_ORDER:
        remote(mid.at[z], mid_in.at[k], pz_s.at[k], pz_r.at[k], at_z(zup[k])).wait_recv()
        low = low + mid_in[k].astype(F32)

    def moments(mean, square, low):
        mean_new = 0.8 * mean + 0.2 * low
        square_new = 0.9 * square + 0.1 * low * low
        return (mean_new, square_new, mean_new / jnp.sqrt(square_new))

    mq_v[...], sqq_v[...], dir_q = moments(qm_v[...], qs_v[...], low[0:8, 0:qcols])
    mo_v[...], soo_v[...], dir_o = moments(om_v[...], os_v[...], low[8:16, :])
    dir_q = jnp.concatenate([dir_q, jnp.zeros((8, 256 - qcols), F32)], axis=1)
    drc[z, y] = jnp.concatenate([dir_q, dir_o], axis=0).astype(BF16)
    z_send(d_blk, dz_s, dz_r)
    y_send(d_blk, dy_s, dy_r, 0)

    outs = []

    def put(src, dst):
        outs.append(pltpu.make_async_copy(src, dst, out_sem.at[len(outs)]))
        outs[-1].start()

    put(mq_v, mean_q)
    put(sqq_v, square_q)
    put(mo_v, mean_o)
    put(soo_v, square_o)

    for k in Z_ORDER:
        z_wait(d_blk, dz_s, dz_r, k)
        y_send(d_blk, dy_s, dy_r, k)
    column = drc[:, y].astype(F32)
    square = column * column
    sum_q = jnp.sum(square[:, 0:8].reshape(64, 256), axis=(0, 1), keepdims=True)
    sum_o = jnp.sum(square[:, 8:16].reshape(64, 256), axis=(0, 1), keepdims=True)
    sums[0] = jnp.concatenate([jnp.broadcast_to(sum_q, (4, 128)), jnp.broadcast_to(sum_o, (4, 128))], axis=0)
    for d in range(1, 8):
        start(remote(sums.at[0], sums_in.at[d], st_s.at[d], st_r.at[d], at_tp(d)))

    for k in order:
        for way in (0, 1):
            y_wait(d_blk, dy_s, dy_r, way, k)
        w_send(d_blk, dw_s, dw_r, k)
    for way in (0, 1):
        row = downs[1] if way == 0 else ups[1]
        src = wei.at[:, row]
        remote(src, src, wy_s.at[way], wy_r.at[way], at_y(row)).wait_recv()
    for i, (lo, row, to) in enumerate(((0, downs[1], ups[1]), (4, ups[1], downs[1]))):
        src = wei.at[pl.ds(lo, 4), row]
        start(remote(src, src, ww_s.at[i], ww_r.at[i], at_y(to)))

    total = sums[0]
    for d in range(1, 8):
        remote(sums.at[0], sums_in.at[d], st_s.at[d], st_r.at[d], at_tp(d)).wait_recv()
        total = total + sums_in[d]
    sums[1] = total
    for d in (1, 2, 3):
        start(remote(sums.at[1], sums_in.at[7 + d], sy_s.at[d], sy_r.at[d], at_y(ups[d])))

    for k in order:
        w_wait(d_blk, dw_s, dw_r, k)
    every = drc[...].astype(F32).reshape(32, 16, 256)
    pq[...] = dot(factor(0, 16), every[:, 0:8].reshape(256, 256).astype(BF16))
    po[...] = dot(factor(16, 32), every[:, 8:16].reshape(256, 256).astype(BF16))
    for d in (1, 2, 3):
        remote(sums.at[1], sums_in.at[7 + d], sy_s.at[d], sy_r.at[d], at_y(ups[d])).wait_recv()
        total = total + sums_in[7 + d]
    count = 256.0 * 8 * qcols
    scale_q = lax.rsqrt(total[0:1, 0:1] / count + 0.25)
    scale_o = lax.rsqrt(total[4:5, 0:1] / (256.0 * 8 * 256) + 0.25)

    own_q = pq[pl.ds(pl.multiple_of(fs * 16, 16), 16), :][:, 0:qcols] * scale_q
    own_o = po[pl.ds(pl.multiple_of(fs * 32, 32), 32), :] * scale_o
    sq_v[...] = own_q
    so_v[...] = own_o
    nq_v[...] = qw_v[...] - 0.02 * own_q
    no_v[...] = ow_v[...] - 0.02 * own_o
    put(sq_v, step_q)
    put(so_v, step_o)
    put(nq_v, new_q)
    put(no_v, new_o)
    for i in (0, 1):
        dst = wei.at[pl.ds(4 * i, 4), ups[2]]
        remote(dst, dst, ww_s.at[i], ww_r.at[i], at_y(ups[1])).wait_recv()
    weights = wei[...].reshape(32, 48, 256).astype(F32)
    weights_q = weights[:, 0:16].reshape(512, 256)
    weights_o = weights[:, 16:48].reshape(1024, 256)
    cq[...] = (weights_q - 0.02 * (pq[...] * scale_q))[:, 0:qcols].astype(BF16)
    put(cq, copy_q)
    co[...] = (weights_o - 0.02 * (po[...] * scale_o)).astype(BF16)
    put(co, copy_o)
    for copy in started:
        copy.wait_send()
    for copy in outs:
        copy.wait()


def solution(mesh):
    def on_device(lat, qcot, att, mix, qw, ow, qf, of, qm, qs, om, os_):
        tokens, qcols = lat.shape[0], qw.shape[1]
        inv_root = 1.0 / math.sqrt(tokens * lax.axis_size("fs"))

        def like(a):
            return jax.ShapeDtypeStruct(a.shape, a.dtype)

        def vm(a):
            return pltpu.VMEM(a.shape, a.dtype)

        dma = pltpu.SemaphoreType.DMA
        any_ = pl.BlockSpec(memory_space=pl.ANY)
        outs = (
            like(qw), like(ow), like(qw), like(ow),
            jax.ShapeDtypeStruct((512, qcols), BF16), jax.ShapeDtypeStruct((1024, 256), BF16),
            like(qm), like(qs), like(om), like(os_),
        )
        return pl.pallas_call(
            functools.partial(kernel, inv_root),
            out_shape=outs,
            in_specs=[any_] * 12,
            out_specs=[any_] * 10,
            scratch_shapes=[
                vm(lat), vm(qcot), vm(att), vm(mix), vm(qw), vm(ow), vm(qm), vm(qs), vm(om), vm(os_),
                pltpu.VMEM((qcols, 512), F32), pltpu.VMEM((256, 1024), F32),
                pltpu.VMEM((2, NZ, NY, 48, 128), BF16), pltpu.VMEM((NZ, NY, 48, 256), BF16),
                pltpu.VMEM((NY, NZ, 16, 256), BF16), pltpu.VMEM((NY, NZ, 16, 256), BF16),
                pltpu.VMEM((NZ, 16, 256), BF16), pltpu.VMEM((NZ, 16, 256), BF16),
                pltpu.VMEM((NZ, NY, 16, 256), BF16),
                pltpu.VMEM((2, 8, 128), F32), pltpu.VMEM((11, 8, 128), F32),
                pltpu.VMEM((512, 256), F32), pltpu.VMEM((1024, 256), F32),
                pltpu.VMEM((512, qcols), BF16), pltpu.VMEM((1024, 256), BF16),
                vm(qw), vm(ow), vm(qw), vm(ow), vm(qm), vm(qs), vm(om), vm(os_),
                dma((CHUNKS, 4)), dma((8,)), dma((10,)),
                dma((8,)), dma((8,)), dma((2, 8)), dma((2, 8)), dma((8,)), dma((8,)), dma((4,)), dma((4,)),
                dma((8,)), dma((8,)), dma((2,)), dma((2,)), dma((2,)), dma((2,)),
                dma((4,)), dma((4,)), dma((8,)), dma((8,)),
                dma((8,)), dma((8,)), dma((2, 8)), dma((2, 8)), dma((8,)), dma((8,)),
                dma((8,)), dma((8,)), dma((4,)), dma((4,)),
            ],
            compiler_params=pltpu.CompilerParams(
                collective_id=0, has_side_effects=True, vmem_limit_bytes=56 * 1024 * 1024
            ),
        )(lat, qcot, att, mix, qw, ow, qf, of, qm, qs, om, os_)

    rows, both, whole = P("fs", None), P("fs", "tp"), P(None, "tp")
    return jax.shard_map(
        on_device,
        mesh=mesh,
        in_specs=(rows, both, rows, both, both, both, rows, rows, both, both, both, both),
        out_specs=(both, both, both, both, whole, whole, both, both, both, both),
        check_vma=False,
    )
```

```python
import functools
import math

import jax
import jax.numpy as jnp
from jax import lax
from jax.experimental import pallas as pl
from jax.experimental.pallas import tpu as pltpu
from jax.sharding import PartitionSpec as P

MESH = pl.DeviceIdType.MESH
F32 = jnp.float32
BF16 = jnp.bfloat16
NZ, NY = 8, 4
CHUNKS = 6
Z_ORDER = (1, 7, 2, 6, 3, 5, 4)
FAR_FIRST = (4, 3, 5, 2, 6, 1, 7)
FORWARD_UP = (0, 7, 6, 5)
FORWARD_DOWN = (1, 2, 3, 4)


def by_tokens(left, right):
    return lax.dot_general(left, right, (((0,), (0,)), ((), ())), preferred_element_type=F32)


def dot(left, right):
    return jnp.dot(left, right, preferred_element_type=F32)


def split_dot(left, right):
    high = left.astype(BF16)
    low = (left - high.astype(F32)).astype(BF16)
    return dot(high, right) + dot(low, right)


def kernel(
    inv_root,
    lat, qcot, att, mix, qw, ow, qf, of, qm, qs, om, os_,
    sq_v, so_v, nq_v, no_v, cq, co, mq_v, sqq_v, mo_v, soo_v,
    lat_v, qcot_v, att_v, mix_v, qw_v, ow_v, qm_v, qs_v, om_v, os_v,
    gq, go, fac, wei, part, part_in, mid, mid_in, drc, sums, sums_in,
    pq, po,
    chunk_sem, small_sem,
    fz_s, fz_r, fy_s, fy_r, fw_s, fw_r, fd_s, fd_r,
    wz_s, wz_r, wy_s, wy_r, ww_s, ww_r,
    py_s, py_r, pz_s, pz_r,
    dz_s, dz_r, dy_s, dy_r, dw_s, dw_r,
    st_s, st_r, sz_s, sz_r, sy_s, sy_r,
):
    fs, tp = lax.axis_index("fs"), lax.axis_index("tp")
    y, z = lax.rem(fs, NY), fs // NY
    core = lax.rem(tp, 2)
    other = 1 - core
    partner = (fs, tp + 1 - 2 * core)
    ups = [lax.rem(y + d, NY) for d in range(NY)]
    downs = [lax.rem(y + NY - d, NY) for d in range(NY)]
    zup = [lax.rem(z + d, NZ) for d in range(NZ)]
    zdn = [lax.rem(z + NZ - d, NZ) for d in range(NZ)]

    def at_y(row):
        return (z * NY + row, tp)

    def at_z(level):
        return (level * NY + y, tp)

    def at_tp(d):
        return (fs, lax.rem(tp + d, 8))

    def remote(src, dst, send, recv, to):
        return pltpu.make_async_remote_copy(
            src_ref=src, dst_ref=dst, send_sem=send, recv_sem=recv, device_id=to, device_id_type=MESH
        )

    barrier = pltpu.get_barrier_semaphore()
    for to in [at_y(ups[d]) for d in range(1, NY)] + [at_z(zup[d]) for d in range(1, NZ)] + [at_tp(d) for d in range(1, 8)]:
        pl.semaphore_signal(barrier, inc=1, device_id=to, device_id_type=MESH)

    half = pl.ds(pl.multiple_of(core * 128, 128), 128)
    own = fac.at[core, z, y]
    small = []
    for i, (src, dst) in enumerate((
        (qf.at[:, half], own.at[pl.ds(0, 16)]),
        (of.at[:, half], own.at[pl.ds(16, 32)]),
        (qw, qw_v), (ow, ow_v), (qm, qm_v), (qs, qs_v), (om, om_v), (os_, os_v),
    )):
        small.append(pltpu.make_async_copy(src, dst, small_sem.at[i]))
        small[-1].start()

    tokens = lat.shape[0]
    rows = tokens // CHUNKS
    pairs = ((lat, lat_v), (mix, mix_v), (att, att_v))

    def chunk_copies(i):
        span = pl.ds(pl.multiple_of(i * rows, rows), rows)
        copies = [
            pltpu.make_async_copy(src.at[span], dst.at[span], chunk_sem.at[i, j])
            for j, (src, dst) in enumerate(pairs)
        ]
        copies.append(pltpu.make_async_copy(qcot.at[:, span], qcot_v.at[:, span], chunk_sem.at[i, 3]))
        return copies

    gq[...] = jnp.zeros_like(gq)
    go[...] = jnp.zeros_like(go)

    def add_chunk(i):
        for copy in chunk_copies(i):
            copy.wait()
        span = pl.ds(pl.multiple_of(i * rows, rows), rows)
        gq[...] += dot(qcot_v[:, span], lat_v[span, :])
        go[...] += by_tokens(mix_v[span, :], att_v[span, :])

    def add_chunks(a, b):
        @pl.loop(a, b)
        def _(i):
            add_chunk(i)

    for copy in small:
        copy.wait()
    for i in range(CHUNKS):
        for copy in chunk_copies(i):
            copy.start()
    qcols = qw_v.shape[1]
    wei[z, y, 0:16, 0:qcols] = qw_v[...].astype(BF16)
    wei[z, y, 16:48, :] = ow_v[...].astype(BF16)

    add_chunks(0, 2)
    pl.semaphore_wait(barrier, 17)

    def f_blk(level, row):
        return fac.at[core, level, row]

    def w_blk(level, row):
        return wei.at[level, row]

    def d_blk(level, row):
        return drc.at[level, row]

    started = []

    def start(copy):
        copy.start()
        started.append(copy)

    def z_send(blk, s, r):
        for k in FAR_FIRST:
            start(remote(blk(z, y), blk(z, y), s.at[k], r.at[k], at_z(zup[k])))

    def z_wait(blk, s, r, k):
        remote(blk(zdn[k], y), blk(zdn[k], y), s.at[k], r.at[k], at_z(zup[k])).wait_recv()

    def y_send(blk, s, r, k):
        for way, row in ((0, ups[1]), (1, downs[1])):
            start(remote(blk(zdn[k], y), blk(zdn[k], y), s.at[way, k], r.at[way, k], at_y(row)))

    def y_wait(blk, s, r, way, k):
        row = downs[1] if way == 0 else ups[1]
        remote(blk(zdn[k], row), blk(zdn[k], row), s.at[way, k], r.at[way, k], at_y(row)).wait_recv()

    def w_send(blk, s, r, k):
        if k in FORWARD_UP:
            src, to = blk(zdn[k], downs[1]), ups[1]
        else:
            src, to = blk(zdn[k], ups[1]), downs[1]
        start(remote(src, src, s.at[k], r.at[k], at_y(to)))

    def w_wait(blk, s, r, k):
        dst = blk(zdn[k], ups[2])
        remote(dst, dst, s.at[k], r.at[k], at_y(ups[1])).wait_recv()

    def swap_send(row, i):
        src = fac.at[core, :, row]
        start(remote(src, src, fd_s.at[i], fd_r.at[i], partner))

    def swap_wait(row, i):
        dst = fac.at[other, :, row]
        remote(dst, dst, fd_s.at[i], fd_r.at[i], partner).wait_recv()

    z_send(f_blk, fz_s, fz_r)
    y_send(f_blk, fy_s, fy_r, 0)
    add_chunks(2, 4)
    for k in Z_ORDER[:4]:
        z_wait(f_blk, fz_s, fz_r, k)
        y_send(f_blk, fy_s, fy_r, k)
    add_chunks(4, CHUNKS)
    for k in Z_ORDER[4:]:
        z_wait(f_blk, fz_s, fz_r, k)
        y_send(f_blk, fy_s, fy_r, k)
    swap_send(y, 0)
    order = (0,) + Z_ORDER
    for k in order[:4]:
        for way in (0, 1):
            y_wait(f_blk, fy_s, fy_r, way, k)
        w_send(f_blk, fw_s, fw_r, k)
    for k in order[4:]:
        for way in (0, 1):
            y_wait(f_blk, fy_s, fy_r, way, k)
        w_send(f_blk, fw_s, fw_r, k)
    swap_send(downs[1], 1)
    swap_send(ups[1], 2)
    z_send(w_blk, wz_s, wz_r)
    for k in order:
        w_wait(f_blk, fw_s, fw_r, k)
    swap_send(ups[2], 3)
    for i, row in enumerate((y, ups[1], downs[1], ups[2])):
        swap_wait(row, i)

    def factor(first, count):
        return jnp.concatenate(
            [fac[c, :, :, first:first + count, :].reshape(32 * count, 128) for c in (0, 1)], axis=1
        )

    low_q = split_dot(gq[...], factor(0, 16)) * inv_root
    low_q = jnp.concatenate([low_q, jnp.zeros((256 - qcols, 256), F32)], axis=0).T
    low_o = (split_dot(go[...], factor(16, 32)) * inv_root).T
    for row in range(NY):
        part[row] = jnp.concatenate(
            [low_q.reshape(NZ, NY, 8, 256)[:, row], low_o.reshape(NZ, NY, 8, 256)[:, row]], axis=1
        ).astype(BF16)

    for d in (2, 1, 3):
        start(remote(part.at[ups[d]], part_in.at[d], py_s.at[d], py_r.at[d], at_y(ups[d])))
    total = part[y].astype(F32)
    for d in (1, 3, 2):
        remote(part.at[y], part_in.at[d], py_s.at[d], py_r.at[d], at_y(ups[d])).wait_recv()
        total = total + part_in[d].astype(F32)
    mid[...] = total.astype(BF16)
    for k in FAR_FIRST:
        start(remote(mid.at[zup[k]], mid_in.at[k], pz_s.at[k], pz_r.at[k], at_z(zup[k])))
    for k in Z_ORDER:
        z_wait(w_blk, wz_s, wz_r, k)
    for way, row in ((0, ups[1]), (1, downs[1])):
        src = wei.at[:, y]
        start(remote(src, src, wy_s.at[way], wy_r.at[way], at_y(row)))
    low = mid[z].astype(F32)
    for k in Z_ORDER:
        remote(mid.at[z], mid_in.at[k], pz_s.at[k], pz_r.at[k], at_z(zup[k])).wait_recv()
        low = low + mid_in[k].astype(F32)

    def moments(mean, square, low):
        mean_new = 0.8 * mean + 0.2 * low
        square_new = 0.9 * square + 0.1 * low * low
        return (mean_new, square_new, mean_new / jnp.sqrt(square_new))

    mq_v[...], sqq_v[...], dir_q = moments(qm_v[...], qs_v[...], low[0:8, 0:qcols])
    mo_v[...], soo_v[...], dir_o = moments(om_v[...], os_v[...], low[8:16, :])
    dir_q = jnp.concatenate([dir_q, jnp.zeros((8, 256 - qcols), F32)], axis=1)
    drc[z, y] = jnp.concatenate([dir_q, dir_o], axis=0).astype(BF16)
    z_send(d_blk, dz_s, dz_r)
    y_send(d_blk, dy_s, dy_r, 0)

    sum_q = jnp.sum(dir_q * dir_q, axis=(0, 1), keepdims=True)
    sum_o = jnp.sum(dir_o * dir_o, axis=(0, 1), keepdims=True)
    sums[0] = jnp.concatenate([jnp.broadcast_to(sum_q, (4, 128)), jnp.broadcast_to(sum_o, (4, 128))], axis=0)
    for d in range(1, 8):
        start(remote(sums.at[0], sums_in.at[d], st_s.at[d], st_r.at[d], at_tp(d)))
    for way in (0, 1):
        row = downs[1] if way == 0 else ups[1]
        src = wei.at[:, row]
        remote(src, src, wy_s.at[way], wy_r.at[way], at_y(row)).wait_recv()
    for i, (lo, row, to) in enumerate(((0, downs[1], ups[1]), (4, ups[1], downs[1]))):
        src = wei.at[pl.ds(lo, 4), row]
        start(remote(src, src, ww_s.at[i], ww_r.at[i], at_y(to)))

    for k in Z_ORDER[:4]:
        z_wait(d_blk, dz_s, dz_r, k)
        y_send(d_blk, dy_s, dy_r, k)
    total = sums[0]
    for d in range(1, 8):
        remote(sums.at[0], sums_in.at[d], st_s.at[d], st_r.at[d], at_tp(d)).wait_recv()
        total = total + sums_in[d]
    sums[1] = total
    for d in FAR_FIRST:
        start(remote(sums.at[1], sums_in.at[7 + d], sz_s.at[d], sz_r.at[d], at_z(zup[d])))
    for k in Z_ORDER[4:]:
        z_wait(d_blk, dz_s, dz_r, k)
        y_send(d_blk, dy_s, dy_r, k)
    for k in order:
        for way in (0, 1):
            y_wait(d_blk, dy_s, dy_r, way, k)
        w_send(d_blk, dw_s, dw_r, k)
    for d in Z_ORDER:
        remote(sums.at[1], sums_in.at[7 + d], sz_s.at[d], sz_r.at[d], at_z(zup[d])).wait_recv()
        total = total + sums_in[7 + d]
    sums[2] = total
    for d in (2, 1, 3):
        start(remote(sums.at[2], sums_in.at[14 + d], sy_s.at[d], sy_r.at[d], at_y(ups[d])))
    for k in order:
        w_wait(d_blk, dw_s, dw_r, k)
    every = drc[...].astype(F32).reshape(32, 16, 256)
    pq[...] = dot(factor(0, 16), every[:, 0:8].reshape(256, 256).astype(BF16))
    po[...] = dot(factor(16, 32), every[:, 8:16].reshape(256, 256).astype(BF16))
    for d in (1, 2, 3):
        remote(sums.at[2], sums_in.at[14 + d], sy_s.at[d], sy_r.at[d], at_y(ups[d])).wait_recv()
        total = total + sums_in[14 + d]
    count = 256.0 * 8 * qcols
    scale_q = lax.rsqrt(total[0:1, 0:1] / count + 0.25)
    scale_o = lax.rsqrt(total[4:5, 0:1] / (256.0 * 8 * 256) + 0.25)

    own_q = pq[pl.ds(pl.multiple_of(fs * 16, 16), 16), :][:, 0:qcols] * scale_q
    own_o = po[pl.ds(pl.multiple_of(fs * 32, 32), 32), :] * scale_o
    sq_v[...] = own_q
    so_v[...] = own_o
    nq_v[...] = qw_v[...] - 0.02 * own_q
    no_v[...] = ow_v[...] - 0.02 * own_o
    for i in (0, 1):
        dst = wei.at[pl.ds(4 * i, 4), ups[2]]
        remote(dst, dst, ww_s.at[i], ww_r.at[i], at_y(ups[1])).wait_recv()
    weights = wei[...].reshape(32, 48, 256).astype(F32)
    weights_q = weights[:, 0:16].reshape(512, 256)
    weights_o = weights[:, 16:48].reshape(1024, 256)
    cq[...] = (weights_q - 0.02 * (pq[...] * scale_q)).T[0:qcols, :].astype(BF16)
    co[...] = (weights_o - 0.02 * (po[...] * scale_o)).astype(BF16)
    for copy in started:
        copy.wait_send()


def write_out(*refs):
    n = len(refs) // 2
    sem = refs[-1]
    copies = [pltpu.make_async_copy(refs[i], refs[n + i], sem.at[i]) for i in range(n)]
    for copy in copies:
        copy.start()
    for copy in copies:
        copy.wait()


def solution(mesh):
    def on_device(lat, qcot, att, mix, qw, ow, qf, of, qm, qs, om, os_):
        tokens, qcols = lat.shape[0], qw.shape[1]
        inv_root = 1.0 / math.sqrt(tokens * lax.axis_size("fs"))

        def like(a):
            return jax.ShapeDtypeStruct(a.shape, a.dtype)

        def vm(a):
            return pltpu.VMEM(a.shape, a.dtype)

        dma = pltpu.SemaphoreType.DMA
        any_ = pl.BlockSpec(memory_space=pl.ANY)
        outs = (
            like(qw), like(ow), like(qw), like(ow),
            jax.ShapeDtypeStruct((qcols, 512), BF16), jax.ShapeDtypeStruct((1024, 256), BF16),
            like(qm), like(qs), like(om), like(os_),
        )
        qcot = qcot.T
        held = pl.pallas_call(
            functools.partial(kernel, inv_root),
            out_shape=[pltpu.VMEM(a.shape, a.dtype) for a in outs],
            in_specs=[any_] * 12,
            out_specs=[pl.BlockSpec(memory_space=pltpu.VMEM)] * 10,
            scratch_shapes=[
                vm(lat), vm(qcot), vm(att), vm(mix), vm(qw), vm(ow), vm(qm), vm(qs), vm(om), vm(os_),
                pltpu.VMEM((qcols, 512), F32), pltpu.VMEM((256, 1024), F32),
                pltpu.VMEM((2, NZ, NY, 48, 128), BF16), pltpu.VMEM((NZ, NY, 48, 256), BF16),
                pltpu.VMEM((NY, NZ, 16, 256), BF16), pltpu.VMEM((NY, NZ, 16, 256), BF16),
                pltpu.VMEM((NZ, 16, 256), BF16), pltpu.VMEM((NZ, 16, 256), BF16),
                pltpu.VMEM((NZ, NY, 16, 256), BF16),
                pltpu.VMEM((3, 8, 128), F32), pltpu.VMEM((18, 8, 128), F32),
                pltpu.VMEM((512, 256), F32), pltpu.VMEM((1024, 256), F32),
                dma((CHUNKS, 4)), dma((8,)),
                dma((8,)), dma((8,)), dma((2, 8)), dma((2, 8)), dma((8,)), dma((8,)), dma((4,)), dma((4,)),
                dma((8,)), dma((8,)), dma((2,)), dma((2,)), dma((2,)), dma((2,)),
                dma((4,)), dma((4,)), dma((8,)), dma((8,)),
                dma((8,)), dma((8,)), dma((2, 8)), dma((2, 8)), dma((8,)), dma((8,)),
                dma((8,)), dma((8,)), dma((8,)), dma((8,)), dma((4,)), dma((4,)),
            ],
            compiler_params=pltpu.CompilerParams(
                collective_id=0, has_side_effects=True, vmem_limit_bytes=56 * 1024 * 1024
            ),
        )(lat, qcot, att, mix, qw, ow, qf, of, qm, qs, om, os_)
        results = pl.pallas_call(
            write_out,
            out_shape=outs,
            in_specs=[pl.BlockSpec(memory_space=pltpu.VMEM)] * 10,
            out_specs=[any_] * 10,
            scratch_shapes=[dma((10,))],
        )(*[pltpu.with_memory_space_constraint(a, pltpu.VMEM) for a in held])
        return (*results[:4], results[4].T, *results[5:])

    rows, both, whole = P("fs", None), P("fs", "tp"), P(None, "tp")
    return jax.shard_map(
        on_device,
        mesh=mesh,
        in_specs=(rows, both, rows, both, both, both, rows, rows, both, both, both, both),
        out_specs=(both, both, both, both, whole, whole, both, both, both, both),
        check_vma=False,
    )
```

```python
import functools
import math

import jax
import jax.numpy as jnp
from jax import lax
from jax.experimental import pallas as pl
from jax.experimental.pallas import tpu as pltpu
from jax.sharding import PartitionSpec as P

MESH = pl.DeviceIdType.MESH
F32 = jnp.float32
BF16 = jnp.bfloat16
NZ, NY = 8, 4
CHUNKS = 6
Z_ORDER = (1, 7, 2, 6, 3, 5, 4)
FAR_FIRST = (4, 3, 5, 2, 6, 1, 7)
SIDE = [(d, e) for d in range(NY) for e in range(8) if d or e]


def by_tokens(left, right):
    return lax.dot_general(left, right, (((0,), (0,)), ((), ())), preferred_element_type=F32)


def dot(left, right):
    return jnp.dot(left, right, preferred_element_type=F32)


def kernel(
    inv_root,
    lat, qcot, att, mix, qw, ow, qf, of, qm, qs, om, os_,
    sq_v, so_v, nq_v, no_v, cq, co, mq_v, sqq_v, mo_v, soo_v,
    lat_v, qcot_v, att_v, mix_v, qw_v, ow_v, qm_v, qs_v, om_v, os_v,
    gq, go, fac, wei, part, part_in, mid, mid_in, drc, sums, sums_in,
    pq, po,
    chunk_sem, small_sem,
    fz_s, fz_r, fy_s, fy_r, fd_s, fd_r,
    wz_s, wz_r, wy_s, wy_r, wb_s, wb_r, wc_s, wc_r,
    py_s, py_r, pz_s, pz_r,
    dz_s, dz_r, dy_s, dy_r,
    sz_s, sz_r,
):
    fs, tp = lax.axis_index("fs"), lax.axis_index("tp")
    y, z = lax.rem(fs, NY), fs // NY
    core = lax.rem(tp, 2)
    other = 1 - core
    partner = (fs, tp + 1 - 2 * core)
    ups = [lax.rem(y + d, NY) for d in range(NY)]
    downs = [lax.rem(y + NY - d, NY) for d in range(NY)]
    zup = [lax.rem(z + d, NZ) for d in range(NZ)]
    zdn = [lax.rem(z + NZ - d, NZ) for d in range(NZ)]

    def at_y(row):
        return (z * NY + row, tp)

    def at_z(level):
        return (level * NY + y, tp)

    def side(d, e):
        return (z * NY + ups[d], lax.rem(tp + e, 8))

    def remote(src, dst, send, recv, to):
        return pltpu.make_async_remote_copy(
            src_ref=src, dst_ref=dst, send_sem=send, recv_sem=recv, device_id=to, device_id_type=MESH
        )

    half = pl.ds(pl.multiple_of(core * 128, 128), 128)
    own = fac.at[core, z, y]
    small = []
    for i, (src, dst) in enumerate((
        (qf.at[:, half], own.at[pl.ds(0, 16)]),
        (of.at[:, half], own.at[pl.ds(16, 32)]),
        (qw, qw_v), (ow, ow_v), (qm, qm_v), (qs, qs_v), (om, om_v), (os_, os_v),
    )):
        small.append(pltpu.make_async_copy(src, dst, small_sem.at[i]))
        small[-1].start()

    barrier = pltpu.get_barrier_semaphore()
    for to in [at_z(zup[d]) for d in range(1, NZ)] + [side(d, e) for d, e in SIDE]:
        pl.semaphore_signal(barrier, inc=1, device_id=to, device_id_type=MESH)

    tokens = lat.shape[0]
    rows = tokens // CHUNKS
    pairs = ((lat, lat_v), (mix, mix_v), (att, att_v))

    def chunk_copies(i):
        span = pl.ds(pl.multiple_of(i * rows, rows), rows)
        copies = [
            pltpu.make_async_copy(src.at[span], dst.at[span], chunk_sem.at[i, j])
            for j, (src, dst) in enumerate(pairs)
        ]
        copies.append(pltpu.make_async_copy(qcot.at[:, span], qcot_v.at[:, span], chunk_sem.at[i, 3]))
        return copies

    def add_chunk(i):
        for copy in chunk_copies(i):
            copy.wait()
        span = pl.ds(pl.multiple_of(i * rows, rows), rows)
        gq[...] += dot(qcot_v[:, span], lat_v[span, :])
        go[...] += by_tokens(mix_v[span, :], att_v[span, :])

    def add_chunks(a, b):
        @pl.loop(a, b)
        def _(i):
            add_chunk(i)

    for copy in small[:4]:
        copy.wait()
    for i in range(CHUNKS):
        for copy in chunk_copies(i):
            copy.start()
    qcols = qw_v.shape[1]
    wei[0, z, y, 0:16] = qw_v[:, 0:128].astype(BF16)
    wei[1, z, y, 0:16, 0:qcols - 128] = qw_v[:, 128:qcols].astype(BF16)
    for i in (0, 1):
        wei[i, z, y, 16:48] = ow_v[:, 128 * i:128 * i + 128].astype(BF16)

    pl.semaphore_wait(barrier, 38)

    def f_blk(level, row):
        return fac.at[core, level, row]

    def w_blk(level, row):
        return wei.at[0, level, row]

    def d_blk(level, row):
        return drc.at[level, row]

    started = []

    def start(copy):
        copy.start()
        started.append(copy)

    def z_send(blk, s, r):
        for k in FAR_FIRST:
            start(remote(blk(z, y), blk(z, y), s.at[k], r.at[k], at_z(zup[k])))

    def z_wait(blk, s, r, k):
        remote(blk(zdn[k], y), blk(zdn[k], y), s.at[k], r.at[k], at_z(zup[k])).wait_recv()

    def y_send(blk, s, r, k):
        for d in (2, 1, 3):
            start(remote(blk(zdn[k], y), blk(zdn[k], y), s.at[d, k], r.at[d, k], at_y(ups[d])))

    def y_wait(blk, s, r, d, k):
        dst = blk(zdn[k], downs[d])
        remote(dst, dst, s.at[d, k], r.at[d, k], at_y(ups[d])).wait_recv()

    def swap_send(d, k):
        src = f_blk(zdn[k], downs[d])
        start(remote(src, src, fd_s.at[d, k], fd_r.at[d, k], partner))

    def swap_wait(d, k):
        dst = fac.at[other, zdn[k], downs[d]]
        remote(dst, dst, fd_s.at[d, k], fd_r.at[d, k], partner).wait_recv()

    z_send(f_blk, fz_s, fz_r)
    y_send(f_blk, fy_s, fy_r, 0)
    swap_send(0, 0)
    for d in (2, 1, 3):
        src = wei.at[1, z, y]
        start(remote(src, src, wb_s.at[d], wb_r.at[d], at_y(ups[d])))
    gq[...] = jnp.zeros_like(gq)
    go[...] = jnp.zeros_like(go)
    add_chunks(0, 4)

    def pass_on(k):
        z_wait(f_blk, fz_s, fz_r, k)
        y_send(f_blk, fy_s, fy_r, k)
        swap_send(0, k)

    for k in Z_ORDER[:2]:
        pass_on(k)
    add_chunks(4, CHUNKS)
    for k in Z_ORDER[2:]:
        pass_on(k)
    z_send(w_blk, wz_s, wz_r)
    for d in (1, 3, 2):
        dst = wei.at[1, z, downs[d]]
        remote(dst, dst, wb_s.at[d], wb_r.at[d], at_y(ups[d])).wait_recv()
    for k in FAR_FIRST:
        src = wei.at[1, z]
        start(remote(src, src, wc_s.at[k], wc_r.at[k], at_z(zup[k])))
    order = (0,) + Z_ORDER
    for k in order:
        for d in (1, 3, 2):
            y_wait(f_blk, fy_s, fy_r, d, k)
            swap_send(d, k)
    for k in order:
        for d in range(NY):
            swap_wait(d, k)

    def factor(first, count):
        return jnp.concatenate(
            [fac[c, :, :, first:first + count, :].reshape(32 * count, 128) for c in (0, 1)], axis=1
        )

    low_q = dot(gq[...].astype(BF16), factor(0, 16)) * inv_root
    low_q = jnp.concatenate([low_q, jnp.zeros((256 - qcols, 256), F32)], axis=0).T
    low_o = (dot(go[...].astype(BF16), factor(16, 32)) * inv_root).T
    low_q, low_o = low_q.reshape(NZ, NY, 8, 256), low_o.reshape(NZ, NY, 8, 256)
    turn = [lax.rem(lev + 2 * NZ - 3 - z, NZ) for lev in range(NZ)]
    for lev in range(NZ):
        for row in range(NY):
            part[row, turn[lev]] = jnp.concatenate([low_q[lev, row], low_o[lev, row]], axis=0).astype(BF16)

    pieces = (pl.ds(0, 3), pl.ds(3, 5))
    for i, piece in enumerate(pieces):
        for d in (2, 1, 3):
            src = part.at[ups[d], piece]
            start(remote(src, part_in.at[d, piece], py_s.at[i, d], py_r.at[i, d], at_y(ups[d])))
    for i, piece in enumerate(pieces):
        total = part[y, piece].astype(F32)
        for d in (1, 3, 2):
            src = part.at[y, piece]
            remote(src, part_in.at[d, piece], py_s.at[i, d], py_r.at[i, d], at_y(ups[d])).wait_recv()
            total = total + part_in[d, piece].astype(F32)
        mid[piece] = total.astype(BF16)
        for k in (4, 3, 5) if i == 0 else (2, 6, 1, 7):
            src = mid.at[(k + NZ - 3) % NZ]
            start(remote(src, mid_in.at[k], pz_s.at[k], pz_r.at[k], at_z(zup[k])))
    for k in Z_ORDER:
        z_wait(w_blk, wz_s, wz_r, k)
    for d in (2, 1, 3):
        src = wei.at[0, :, y]
        start(remote(src, src, wy_s.at[d], wy_r.at[d], at_y(ups[d])))
    low = mid[5].astype(F32)
    for k in Z_ORDER:
        remote(mid.at[5], mid_in.at[k], pz_s.at[k], pz_r.at[k], at_z(zup[k])).wait_recv()
        low = low + mid_in[k].astype(F32)

    def moments(mean, square, low):
        mean_new = 0.8 * mean + 0.2 * low
        square_new = 0.9 * square + 0.1 * low * low
        return (mean_new, square_new, mean_new / jnp.sqrt(square_new))

    for copy in small[4:]:
        copy.wait()
    mq_v[...], sqq_v[...], dir_q = moments(qm_v[...], qs_v[...], low[0:8, 0:qcols])
    mo_v[...], soo_v[...], dir_o = moments(om_v[...], os_v[...], low[8:16, :])
    dir_q = jnp.concatenate([dir_q, jnp.zeros((8, 256 - qcols), F32)], axis=1)
    drc[z, y] = jnp.concatenate([dir_q, dir_o], axis=0).astype(BF16)
    sent = len(started) - 3
    z_send(d_blk, dz_s, dz_r)
    y_send(d_blk, dy_s, dy_r, 0)

    def squares(rows):
        both = rows.astype(F32)
        return both * both

    for copy in started[:sent]:
        copy.wait_send()
    square = squares(drc[z, y])
    for k in Z_ORDER[:4]:
        z_wait(d_blk, dz_s, dz_r, k)
        y_send(d_blk, dy_s, dy_r, k)
        square = square + squares(drc[zdn[k], y])
    for k in Z_ORDER[4:]:
        z_wait(d_blk, dz_s, dz_r, k)
        y_send(d_blk, dy_s, dy_r, k)
    for k in Z_ORDER[4:]:
        square = square + squares(drc[zdn[k], y])
    sum_q = jnp.sum(square[0:8], axis=(0, 1), keepdims=True)
    sum_o = jnp.sum(square[8:16], axis=(0, 1), keepdims=True)
    sums[0] = jnp.concatenate([jnp.broadcast_to(sum_q, (1, 64)), jnp.broadcast_to(sum_o, (1, 64))], axis=1)
    for i, (d, e) in enumerate(SIDE):
        start(remote(sums.at[0], sums_in.at[i], sz_s.at[i], sz_r.at[i], side(d, e)))
    for k in order:
        for d in (1, 3, 2):
            y_wait(d_blk, dy_s, dy_r, d, k)
    every = drc[...].astype(F32).reshape(32, 16, 256)
    pq[...] = dot(factor(0, 16), every[:, 0:8].reshape(256, 256).astype(BF16))
    po[...] = dot(factor(16, 32), every[:, 8:16].reshape(256, 256).astype(BF16))
    total = sums[0]
    for i in range(31):
        remote(sums.at[0], sums_in.at[i], sz_s.at[i], sz_r.at[i], partner).wait_recv()
        total = total + sums_in[i]
    count = 256.0 * 8 * qcols
    scale_q = lax.rsqrt(total[0:1, 0:1] / count + 0.25)
    scale_o = lax.rsqrt(total[0:1, 64:65] / (256.0 * 8 * 256) + 0.25)

    own_q = pq[pl.ds(pl.multiple_of(fs * 16, 16), 16), :][:, 0:qcols] * scale_q
    own_o = po[pl.ds(pl.multiple_of(fs * 32, 32), 32), :] * scale_o
    sq_v[...] = own_q
    so_v[...] = own_o
    nq_v[...] = qw_v[...] - 0.02 * own_q
    no_v[...] = ow_v[...] - 0.02 * own_o
    for d in (1, 3, 2):
        dst = wei.at[0, :, downs[d]]
        remote(dst, dst, wy_s.at[d], wy_r.at[d], at_y(ups[d])).wait_recv()
    for k in Z_ORDER:
        dst = wei.at[1, zdn[k]]
        remote(dst, dst, wc_s.at[k], wc_r.at[k], at_z(zup[k])).wait_recv()
    weights = jnp.concatenate([wei[0].reshape(32, 48, 128), wei[1].reshape(32, 48, 128)], axis=2).astype(F32)
    weights_q = weights[:, 0:16].reshape(512, 256)
    weights_o = weights[:, 16:48].reshape(1024, 256)
    cq[...] = (weights_q - 0.02 * (pq[...] * scale_q)).T[0:qcols, :].astype(BF16)
    co[...] = (weights_o - 0.02 * (po[...] * scale_o)).astype(BF16)
    for copy in started[sent:]:
        copy.wait_send()


def write_out(*refs):
    n = len(refs) // 2
    sem = refs[-1]
    copies = [pltpu.make_async_copy(refs[i], refs[n + i], sem.at[i]) for i in range(n)]
    for copy in copies:
        copy.start()
    for copy in copies:
        copy.wait()


def solution(mesh):
    def on_device(lat, qcot, att, mix, qw, ow, qf, of, qm, qs, om, os_):
        tokens, qcols = lat.shape[0], qw.shape[1]
        inv_root = 1.0 / math.sqrt(tokens * lax.axis_size("fs"))

        def like(a):
            return jax.ShapeDtypeStruct(a.shape, a.dtype)

        def vm(a):
            return pltpu.VMEM(a.shape, a.dtype)

        dma = pltpu.SemaphoreType.DMA
        any_ = pl.BlockSpec(memory_space=pl.ANY)
        outs = (
            like(qw), like(ow), like(qw), like(ow),
            jax.ShapeDtypeStruct((qcols, 512), BF16), jax.ShapeDtypeStruct((1024, 256), BF16),
            like(qm), like(qs), like(om), like(os_),
        )
        qcot = qcot.T
        held = pl.pallas_call(
            functools.partial(kernel, inv_root),
            out_shape=[pltpu.VMEM(a.shape, a.dtype) for a in outs],
            in_specs=[any_] * 12,
            out_specs=[pl.BlockSpec(memory_space=pltpu.VMEM)] * 10,
            scratch_shapes=[
                vm(lat), vm(qcot), vm(att), vm(mix), vm(qw), vm(ow), vm(qm), vm(qs), vm(om), vm(os_),
                pltpu.VMEM((qcols, 512), F32), pltpu.VMEM((256, 1024), F32),
                pltpu.VMEM((2, NZ, NY, 48, 128), BF16), pltpu.VMEM((2, NZ, NY, 48, 128), BF16),
                pltpu.VMEM((NY, NZ, 16, 256), BF16), pltpu.VMEM((NY, NZ, 16, 256), BF16),
                pltpu.VMEM((NZ, 16, 256), BF16), pltpu.VMEM((NZ, 16, 256), BF16),
                pltpu.VMEM((NZ, NY, 16, 256), BF16),
                pltpu.VMEM((1, 1, 128), F32), pltpu.VMEM((31, 1, 128), F32),
                pltpu.VMEM((512, 256), F32), pltpu.VMEM((1024, 256), F32),
                dma((CHUNKS, 4)), dma((8,)),
                dma((8,)), dma((8,)), dma((4, 8)), dma((4, 8)), dma((4, 8)), dma((4, 8)),
                dma((8,)), dma((8,)), dma((4,)), dma((4,)), dma((4,)), dma((4,)), dma((8,)), dma((8,)),
                dma((2, 4)), dma((2, 4)), dma((8,)), dma((8,)),
                dma((8,)), dma((8,)), dma((4, 8)), dma((4, 8)),
                dma((31,)), dma((31,)),
            ],
            compiler_params=pltpu.CompilerParams(
                collective_id=0, has_side_effects=True, vmem_limit_bytes=56 * 1024 * 1024
            ),
        )(lat, qcot, att, mix, qw, ow, qf, of, qm, qs, om, os_)
        results = pl.pallas_call(
            write_out,
            out_shape=outs,
            in_specs=[pl.BlockSpec(memory_space=pltpu.VMEM)] * 10,
            out_specs=[any_] * 10,
            scratch_shapes=[dma((10,))],
        )(*[pltpu.with_memory_space_constraint(a, pltpu.VMEM) for a in held])
        return (*results[:4], results[4].T, *results[5:])

    rows, both, whole = P("fs", None), P("fs", "tp"), P(None, "tp")
    return jax.shard_map(
        on_device,
        mesh=mesh,
        in_specs=(rows, both, rows, both, both, both, rows, rows, both, both, both, both),
        out_specs=(both, both, both, both, whole, whole, both, both, both, both),
        check_vma=False,
    )
```

```python
import functools
import math

import jax
import jax.numpy as jnp
from jax import lax
from jax.experimental import pallas as pl
from jax.experimental.pallas import tpu as pltpu
from jax.sharding import PartitionSpec as P

MESH = pl.DeviceIdType.MESH
F32 = jnp.float32
BF16 = jnp.bfloat16
NZ, NY = 8, 4
CHUNKS = 6
Z_ORDER = (1, 7, 2, 6, 3, 5, 4)
FAR_FIRST = (4, 3, 5, 2, 6, 1, 7)
SIDE = [(d, e) for d in range(NY) for e in range(8) if d or e]


def by_tokens(left, right):
    return lax.dot_general(left, right, (((0,), (0,)), ((), ())), preferred_element_type=F32)


def dot(left, right):
    return jnp.dot(left, right, preferred_element_type=F32)


def kernel(
    inv_root,
    lat, qcot, att, mix, qw, ow, qf, of, qm, qs, om, os_,
    sq_v, so_v, nq_v, no_v, cq, co, mq_v, sqq_v, mo_v, soo_v,
    lat_v, qcot_v, att_v, mix_v, qw_v, ow_v, qm_v, qs_v, om_v, os_v,
    gq, go, fac, wei, part, part_in, mid, mid_in, drc, sums, sums_in,
    pq, po,
    chunk_sem, small_sem,
    fz_s, fz_r, fy_s, fy_r, fd_s, fd_r,
    wz_s, wz_r, wy_s, wy_r, wb_s, wb_r, wc_s, wc_r,
    py_s, py_r, pz_s, pz_r,
    dz_s, dz_r, dy_s, dy_r,
    sx_s, sx_r, sz_s, sz_r,
):
    fs, tp = lax.axis_index("fs"), lax.axis_index("tp")
    y, z = lax.rem(fs, NY), fs // NY
    core = lax.rem(tp, 2)
    other = 1 - core
    partner = (fs, tp + 1 - 2 * core)
    ups = [lax.rem(y + d, NY) for d in range(NY)]
    downs = [lax.rem(y + NY - d, NY) for d in range(NY)]
    zup = [lax.rem(z + d, NZ) for d in range(NZ)]
    zdn = [lax.rem(z + NZ - d, NZ) for d in range(NZ)]

    def at_y(row):
        return (z * NY + row, tp)

    def at_z(level):
        return (level * NY + y, tp)

    def side(d, e):
        return (z * NY + ups[d], lax.rem(tp + e, 8))

    def remote(src, dst, send, recv, to):
        return pltpu.make_async_remote_copy(
            src_ref=src, dst_ref=dst, send_sem=send, recv_sem=recv, device_id=to, device_id_type=MESH
        )

    half = pl.ds(pl.multiple_of(core * 128, 128), 128)
    own = fac.at[core, z, y]
    small = []
    for i, (src, dst) in enumerate((
        (qf.at[:, half], own.at[pl.ds(0, 16)]),
        (of.at[:, half], own.at[pl.ds(16, 32)]),
        (qw, qw_v), (ow, ow_v), (qm, qm_v), (qs, qs_v), (om, om_v), (os_, os_v),
    )):
        small.append(pltpu.make_async_copy(src, dst, small_sem.at[i]))
        small[-1].start()

    barrier = pltpu.get_barrier_semaphore()
    for to in [at_z(zup[d]) for d in range(1, NZ)] + [side(d, e) for d, e in SIDE]:
        pl.semaphore_signal(barrier, inc=1, device_id=to, device_id_type=MESH)

    tokens = lat.shape[0]
    rows = tokens // CHUNKS
    pairs = ((lat, lat_v), (mix, mix_v), (att, att_v))

    def chunk_copies(i):
        span = pl.ds(pl.multiple_of(i * rows, rows), rows)
        copies = [
            pltpu.make_async_copy(src.at[span], dst.at[span], chunk_sem.at[i, j])
            for j, (src, dst) in enumerate(pairs)
        ]
        copies.append(pltpu.make_async_copy(qcot.at[:, span], qcot_v.at[:, span], chunk_sem.at[i, 3]))
        return copies

    def add_chunk(i):
        for copy in chunk_copies(i):
            copy.wait()
        span = pl.ds(pl.multiple_of(i * rows, rows), rows)
        gq[...] += dot(qcot_v[:, span], lat_v[span, :])
        go[...] += by_tokens(mix_v[span, :], att_v[span, :])

    def add_chunks(a, b):
        @pl.loop(a, b)
        def _(i):
            add_chunk(i)

    for copy in small[:4]:
        copy.wait()
    for i in range(CHUNKS):
        for copy in chunk_copies(i):
            copy.start()
    qcols = qw_v.shape[1]
    wei[0, z, y, 0:16] = qw_v[:, 0:128].astype(BF16)
    wei[1, z, y, 0:16, 0:qcols - 128] = qw_v[:, 128:qcols].astype(BF16)
    for i in (0, 1):
        wei[i, z, y, 16:48] = ow_v[:, 128 * i:128 * i + 128].astype(BF16)

    pl.semaphore_wait(barrier, 38)

    def f_blk(level, row):
        return fac.at[core, level, row]

    def w_blk(level, row):
        return wei.at[0, level, row]

    def d_blk(level, row):
        return drc.at[level, row]

    started = []

    def start(copy):
        copy.start()
        started.append(copy)

    def z_send(blk, s, r):
        for k in FAR_FIRST:
            start(remote(blk(z, y), blk(z, y), s.at[k], r.at[k], at_z(zup[k])))

    def z_wait(blk, s, r, k):
        remote(blk(zdn[k], y), blk(zdn[k], y), s.at[k], r.at[k], at_z(zup[k])).wait_recv()

    def y_send(blk, s, r, k):
        for d in (2, 1, 3):
            start(remote(blk(zdn[k], y), blk(zdn[k], y), s.at[d, k], r.at[d, k], at_y(ups[d])))

    def y_wait(blk, s, r, d, k):
        dst = blk(zdn[k], downs[d])
        remote(dst, dst, s.at[d, k], r.at[d, k], at_y(ups[d])).wait_recv()

    def swap_send(d, k):
        src = f_blk(zdn[k], downs[d])
        start(remote(src, src, fd_s.at[d, k], fd_r.at[d, k], partner))

    def swap_wait(d, k):
        dst = fac.at[other, zdn[k], downs[d]]
        remote(dst, dst, fd_s.at[d, k], fd_r.at[d, k], partner).wait_recv()

    z_send(f_blk, fz_s, fz_r)
    y_send(f_blk, fy_s, fy_r, 0)
    swap_send(0, 0)
    for d in (2, 1, 3):
        src = wei.at[1, z, y]
        start(remote(src, src, wb_s.at[d], wb_r.at[d], at_y(ups[d])))
    gq[...] = jnp.zeros_like(gq)
    go[...] = jnp.zeros_like(go)

    def pass_on(k):
        z_wait(f_blk, fz_s, fz_r, k)
        y_send(f_blk, fy_s, fy_r, k)
        swap_send(0, k)

    add_chunks(0, 3)
    for k in Z_ORDER[:2]:
        pass_on(k)
    add_chunks(3, 4)
    for k in Z_ORDER[2:4]:
        pass_on(k)
    add_chunks(4, 5)
    for k in Z_ORDER[4:]:
        pass_on(k)
    add_chunks(5, 6)
    z_send(w_blk, wz_s, wz_r)
    for d in (1, 3, 2):
        dst = wei.at[1, z, downs[d]]
        remote(dst, dst, wb_s.at[d], wb_r.at[d], at_y(ups[d])).wait_recv()
    for k in FAR_FIRST:
        src = wei.at[1, z]
        start(remote(src, src, wc_s.at[k], wc_r.at[k], at_z(zup[k])))
    order = (0,) + Z_ORDER
    for k in order:
        for d in (1, 3, 2):
            y_wait(f_blk, fy_s, fy_r, d, k)
            swap_send(d, k)
    for k in order:
        for d in range(NY):
            swap_wait(d, k)

    def factor(first, count):
        return jnp.concatenate(
            [fac[c, :, :, first:first + count, :].reshape(32 * count, 128) for c in (0, 1)], axis=1
        )

    low_q = dot(gq[...].astype(BF16), factor(0, 16)) * inv_root
    low_q = jnp.concatenate([low_q, jnp.zeros((256 - qcols, 256), F32)], axis=0).T
    low_o = (dot(go[...].astype(BF16), factor(16, 32)) * inv_root).T
    low_q, low_o = low_q.reshape(NZ, NY, 8, 256), low_o.reshape(NZ, NY, 8, 256)
    turn = [lax.rem(lev + 2 * NZ - 3 - z, NZ) for lev in range(NZ)]
    for lev in range(NZ):
        for row in range(NY):
            part[row, turn[lev]] = jnp.concatenate([low_q[lev, row], low_o[lev, row]], axis=0).astype(BF16)

    pieces = (pl.ds(0, 3), pl.ds(3, 5))
    for i, piece in enumerate(pieces):
        for d in (2, 1, 3):
            src = part.at[ups[d], piece]
            start(remote(src, part_in.at[d, piece], py_s.at[i, d], py_r.at[i, d], at_y(ups[d])))
    for i, piece in enumerate(pieces):
        total = part[y, piece].astype(F32)
        for d in (1, 3, 2):
            src = part.at[y, piece]
            remote(src, part_in.at[d, piece], py_s.at[i, d], py_r.at[i, d], at_y(ups[d])).wait_recv()
            total = total + part_in[d, piece].astype(F32)
        mid[piece] = total.astype(BF16)
        for k in (4, 3, 5) if i == 0 else (2, 6, 1, 7):
            src = mid.at[(k + NZ - 3) % NZ]
            start(remote(src, mid_in.at[k], pz_s.at[k], pz_r.at[k], at_z(zup[k])))
    for k in Z_ORDER:
        z_wait(w_blk, wz_s, wz_r, k)
    for d in (2, 1, 3):
        src = wei.at[0, :, y]
        start(remote(src, src, wy_s.at[d], wy_r.at[d], at_y(ups[d])))
    low = mid[5].astype(F32)
    for k in Z_ORDER:
        remote(mid.at[5], mid_in.at[k], pz_s.at[k], pz_r.at[k], at_z(zup[k])).wait_recv()
        low = low + mid_in[k].astype(F32)

    def moments(mean, square, low):
        mean_new = 0.8 * mean + 0.2 * low
        square_new = 0.9 * square + 0.1 * low * low
        return (mean_new, square_new, mean_new / jnp.sqrt(square_new))

    for copy in small[4:]:
        copy.wait()
    mq_v[...], sqq_v[...], dir_q = moments(qm_v[...], qs_v[...], low[0:8, 0:qcols])
    mo_v[...], soo_v[...], dir_o = moments(om_v[...], os_v[...], low[8:16, :])
    dir_q = jnp.concatenate([dir_q, jnp.zeros((8, 256 - qcols), F32)], axis=1)
    drc[z, y] = jnp.concatenate([dir_q, dir_o], axis=0).astype(BF16)
    sent = len(started) - 3
    z_send(d_blk, dz_s, dz_r)
    y_send(d_blk, dy_s, dy_r, 0)

    sum_q = jnp.sum(dir_q * dir_q, axis=(0, 1), keepdims=True)
    sum_o = jnp.sum(dir_o * dir_o, axis=(0, 1), keepdims=True)
    sums[0] = jnp.concatenate([jnp.broadcast_to(sum_q, (1, 64)), jnp.broadcast_to(sum_o, (1, 64))], axis=1)
    for i, (d, e) in enumerate(SIDE):
        start(remote(sums.at[0], sums_in.at[i], sx_s.at[i], sx_r.at[i], side(d, e)))
    for copy in started[:sent]:
        copy.wait_send()
    for k in Z_ORDER[:4]:
        z_wait(d_blk, dz_s, dz_r, k)
        y_send(d_blk, dy_s, dy_r, k)
    for k in Z_ORDER[4:]:
        z_wait(d_blk, dz_s, dz_r, k)
        y_send(d_blk, dy_s, dy_r, k)
    total = sums[0]
    for i in range(31):
        remote(sums.at[0], sums_in.at[i], sx_s.at[i], sx_r.at[i], partner).wait_recv()
        total = total + sums_in[i]
    sums[1] = total

    def sum_copies():
        return [
            remote(sums.at[1], sums_in.at[31 + k], sz_s.at[c, k], sz_r.at[k], (zup[k] * NY + y, tp - c))
            for k in FAR_FIRST
            for c in (1, 0)
        ]

    @pl.when(core == 1)
    def _():
        for copy in sum_copies():
            copy.start()

    for k in order:
        for d in (1, 3, 2):
            y_wait(d_blk, dy_s, dy_r, d, k)
    every = drc[...].astype(F32).reshape(32, 16, 256)
    pq[...] = dot(factor(0, 16), every[:, 0:8].reshape(256, 256).astype(BF16))
    po[...] = dot(factor(16, 32), every[:, 8:16].reshape(256, 256).astype(BF16))
    for k in Z_ORDER:
        remote(sums.at[1], sums_in.at[31 + k], sz_s.at[0, k], sz_r.at[k], at_z(zup[k])).wait_recv()
        total = total + sums_in[31 + k]
    count = 256.0 * 8 * qcols
    scale_q = lax.rsqrt(total[0:1, 0:1] / count + 0.25)
    scale_o = lax.rsqrt(total[0:1, 64:65] / (256.0 * 8 * 256) + 0.25)

    own_q = pq[pl.ds(pl.multiple_of(fs * 16, 16), 16), :][:, 0:qcols] * scale_q
    own_o = po[pl.ds(pl.multiple_of(fs * 32, 32), 32), :] * scale_o
    sq_v[...] = own_q
    so_v[...] = own_o
    nq_v[...] = qw_v[...] - 0.02 * own_q
    no_v[...] = ow_v[...] - 0.02 * own_o
    for d in (1, 3, 2):
        dst = wei.at[0, :, downs[d]]
        remote(dst, dst, wy_s.at[d], wy_r.at[d], at_y(ups[d])).wait_recv()
    for k in Z_ORDER:
        dst = wei.at[1, zdn[k]]
        remote(dst, dst, wc_s.at[k], wc_r.at[k], at_z(zup[k])).wait_recv()
    weights = jnp.concatenate([wei[0].reshape(32, 48, 128), wei[1].reshape(32, 48, 128)], axis=2).astype(F32)
    weights_q = weights[:, 0:16].reshape(512, 256)
    weights_o = weights[:, 16:48].reshape(1024, 256)
    cq[...] = (weights_q - 0.02 * (pq[...] * scale_q)).T[0:qcols, :].astype(BF16)
    co[...] = (weights_o - 0.02 * (po[...] * scale_o)).astype(BF16)
    for copy in started[sent:]:
        copy.wait_send()

    @pl.when(core == 1)
    def _():
        for copy in sum_copies():
            copy.wait_send()


def write_out(*refs):
    n = len(refs) // 2
    sem = refs[-1]
    copies = [pltpu.make_async_copy(refs[i], refs[n + i], sem.at[i]) for i in range(n)]
    for copy in copies:
        copy.start()
    for copy in copies:
        copy.wait()


def solution(mesh):
    def on_device(lat, qcot, att, mix, qw, ow, qf, of, qm, qs, om, os_):
        tokens, qcols = lat.shape[0], qw.shape[1]
        inv_root = 1.0 / math.sqrt(tokens * lax.axis_size("fs"))

        def like(a):
            return jax.ShapeDtypeStruct(a.shape, a.dtype)

        def vm(a):
            return pltpu.VMEM(a.shape, a.dtype)

        dma = pltpu.SemaphoreType.DMA
        any_ = pl.BlockSpec(memory_space=pl.ANY)
        outs = (
            like(qw), like(ow), like(qw), like(ow),
            jax.ShapeDtypeStruct((qcols, 512), BF16), jax.ShapeDtypeStruct((1024, 256), BF16),
            like(qm), like(qs), like(om), like(os_),
        )
        qcot = qcot.T
        held = pl.pallas_call(
            functools.partial(kernel, inv_root),
            out_shape=[pltpu.VMEM(a.shape, a.dtype) for a in outs],
            in_specs=[any_] * 12,
            out_specs=[pl.BlockSpec(memory_space=pltpu.VMEM)] * 10,
            scratch_shapes=[
                vm(lat), vm(qcot), vm(att), vm(mix), vm(qw), vm(ow), vm(qm), vm(qs), vm(om), vm(os_),
                pltpu.VMEM((qcols, 512), F32), pltpu.VMEM((256, 1024), F32),
                pltpu.VMEM((2, NZ, NY, 48, 128), BF16), pltpu.VMEM((2, NZ, NY, 48, 128), BF16),
                pltpu.VMEM((NY, NZ, 16, 256), BF16), pltpu.VMEM((NY, NZ, 16, 256), BF16),
                pltpu.VMEM((NZ, 16, 256), BF16), pltpu.VMEM((NZ, 16, 256), BF16),
                pltpu.VMEM((NZ, NY, 16, 256), BF16),
                pltpu.VMEM((2, 1, 128), F32), pltpu.VMEM((39, 1, 128), F32),
                pltpu.VMEM((512, 256), F32), pltpu.VMEM((1024, 256), F32),
                dma((CHUNKS, 4)), dma((8,)),
                dma((8,)), dma((8,)), dma((4, 8)), dma((4, 8)), dma((4, 8)), dma((4, 8)),
                dma((8,)), dma((8,)), dma((4,)), dma((4,)), dma((4,)), dma((4,)), dma((8,)), dma((8,)),
                dma((2, 4)), dma((2, 4)), dma((8,)), dma((8,)),
                dma((8,)), dma((8,)), dma((4, 8)), dma((4, 8)),
                dma((31,)), dma((31,)), dma((2, 8)), dma((8,)),
            ],
            compiler_params=pltpu.CompilerParams(
                collective_id=0, has_side_effects=True, vmem_limit_bytes=56 * 1024 * 1024
            ),
        )(lat, qcot, att, mix, qw, ow, qf, of, qm, qs, om, os_)
        results = pl.pallas_call(
            write_out,
            out_shape=outs,
            in_specs=[pl.BlockSpec(memory_space=pltpu.VMEM)] * 10,
            out_specs=[any_] * 10,
            scratch_shapes=[dma((10,))],
        )(*[pltpu.with_memory_space_constraint(a, pltpu.VMEM) for a in held])
        return (*results[:4], results[4].T, *results[5:])

    rows, both, whole = P("fs", None), P("fs", "tp"), P(None, "tp")
    return jax.shard_map(
        on_device,
        mesh=mesh,
        in_specs=(rows, both, rows, both, both, both, rows, rows, both, both, both, both),
        out_specs=(both, both, both, both, whole, whole, both, both, both, both),
        check_vma=False,
    )
```

```python
import functools
import math

import jax
import jax.numpy as jnp
from jax import lax
from jax.experimental import pallas as pl
from jax.experimental.pallas import tpu as pltpu
from jax.sharding import PartitionSpec as P

MESH = pl.DeviceIdType.MESH
F32 = jnp.float32
BF16 = jnp.bfloat16
NZ, NY = 8, 4
CHUNKS = 6
Z_ORDER = (1, 7, 2, 6, 3, 5, 4)
FAR_FIRST = (4, 3, 5, 2, 6, 1, 7)
BY_DISTANCE = (4, 3, 5, 2, 6, 1, 7, 0)
PIECES = ((0, 1), (1, 2), (3, 2), (5, 3))
SIDE = [(d, e) for d in range(NY) for e in range(8) if d or e]


def by_tokens(left, right):
    return lax.dot_general(left, right, (((0,), (0,)), ((), ())), preferred_element_type=F32)


def dot(left, right):
    return jnp.dot(left, right, preferred_element_type=F32)


def kernel(
    inv_root,
    lat, qcot, att, mix, qw, ow, qf, of, qm, qs, om, os_,
    sq_v, so_v, nq_v, no_v, cq, co, mq_v, sqq_v, mo_v, soo_v,
    lat_v, qcot_v, att_v, mix_v, qw_v, ow_v, qm_v, qs_v, om_v, os_v,
    gq, go, fac, wei, part, part_in, mid, mid_in, drc, sums, sums_in,
    pq, po,
    chunk_sem, small_sem,
    fz_s, fz_r, fy_s, fy_r, fd_s, fd_r,
    wz_s, wz_r, wy_s, wy_r, wb_s, wb_r, wc_s, wc_r,
    py_s, py_r, pz_s, pz_r,
    dz_s, dz_r, dy_s, dy_r,
    sx_s, sx_r, sz_s, sz_r, met,
):
    fs, tp = lax.axis_index("fs"), lax.axis_index("tp")
    y, z = lax.rem(fs, NY), fs // NY
    core = lax.rem(tp, 2)
    other = 1 - core
    partner = (fs, tp + 1 - 2 * core)
    ups = [lax.rem(y + d, NY) for d in range(NY)]
    downs = [lax.rem(y + NY - d, NY) for d in range(NY)]
    zup = [lax.rem(z + d, NZ) for d in range(NZ)]
    zdn = [lax.rem(z + NZ - d, NZ) for d in range(NZ)]

    def at_y(row):
        return (z * NY + row, tp)

    def at_z(level):
        return (level * NY + y, tp)

    def side(d, e):
        return (z * NY + ups[d], lax.rem(tp + e, 8))

    def remote(src, dst, send, recv, to):
        return pltpu.make_async_remote_copy(
            src_ref=src, dst_ref=dst, send_sem=send, recv_sem=recv, device_id=to, device_id_type=MESH
        )

    half = pl.ds(pl.multiple_of(core * 128, 128), 128)
    own = fac.at[core, z, y]
    small = []
    for i, (src, dst) in enumerate((
        (qf.at[:, half], own.at[pl.ds(0, 16)]),
        (of.at[:, half], own.at[pl.ds(16, 32)]),
        (qw, qw_v), (ow, ow_v), (qm, qm_v), (qs, qs_v), (om, om_v), (os_, os_v),
    )):
        small.append(pltpu.make_async_copy(src, dst, small_sem.at[i]))
        small[-1].start()

    across = [(fs, lax.rem(tp + e, 8)) for e in (4, 2, 6)]
    barrier = pltpu.get_barrier_semaphore()
    for to in [at_z(zup[k]) for k in FAR_FIRST] + [at_y(ups[d]) for d in (2, 1, 3)] + [partner] + across:
        pl.semaphore_signal(barrier, inc=1, device_id=to, device_id_type=MESH)

    tokens = lat.shape[0]
    rows = tokens // CHUNKS
    pairs = ((lat, lat_v), (mix, mix_v), (att, att_v))

    def chunk_copies(i):
        span = pl.ds(pl.multiple_of(i * rows, rows), rows)
        copies = [
            pltpu.make_async_copy(src.at[span], dst.at[span], chunk_sem.at[i, j])
            for j, (src, dst) in enumerate(pairs)
        ]
        copies.append(pltpu.make_async_copy(qcot.at[:, span], qcot_v.at[:, span], chunk_sem.at[i, 3]))
        return copies

    def add_chunk(i):
        for copy in chunk_copies(i):
            copy.wait()
        span = pl.ds(pl.multiple_of(i * rows, rows), rows)
        gq[...] += dot(qcot_v[:, span], lat_v[span, :])
        go[...] += by_tokens(mix_v[span, :], att_v[span, :])

    def add_chunks(a, b):
        @pl.loop(a, b)
        def _(i):
            add_chunk(i)

    for copy in small[:4]:
        copy.wait()
    for i in range(CHUNKS):
        for copy in chunk_copies(i):
            copy.start()
    qcols = qw_v.shape[1]
    wei[0, z, y, 0:16] = qw_v[:, 0:128].astype(BF16)
    wei[1, z, y, 0:16, 0:qcols - 128] = qw_v[:, 128:qcols].astype(BF16)
    for i in (0, 1):
        wei[i, z, y, 16:48] = ow_v[:, 128 * i:128 * i + 128].astype(BF16)

    pl.semaphore_wait(barrier, 14)

    def f_blk(level, row):
        return fac.at[core, level, row]

    def w_blk(level, row):
        return wei.at[0, level, row]

    def d_blk(level, row):
        return drc.at[level, row]

    def start(copy):
        copy.start()

    def arrived(ref, sem):
        pltpu.make_async_copy(ref, ref, sem).wait()

    sent = arrived

    def z_send(blk, s, r):
        for k in FAR_FIRST:
            start(remote(blk(z, y), blk(z, y), s, r.at[k], at_z(zup[k])))

    def z_wait(blk, r, k):
        arrived(blk(zdn[k], y), r.at[k])

    def y_send(blk, s, r, k):
        for d in (2, 1, 3):
            start(remote(blk(zdn[k], y), blk(zdn[k], y), s, r(k), at_y(ups[d])))

    def swap_send(d, k):
        src = f_blk(zdn[k], downs[d])
        start(remote(src, src, fd_s, fd_r, partner))

    z_send(f_blk, fz_s, fz_r)
    y_send(f_blk, fy_s, fy_r.at.__getitem__, 0)
    swap_send(0, 0)
    for d in (2, 1, 3):
        src = wei.at[1, z, y]
        start(remote(src, src, wb_s, wb_r, at_y(ups[d])))
    gq[...] = jnp.zeros_like(gq)
    go[...] = jnp.zeros_like(go)

    def pass_on(k):
        z_wait(f_blk, fz_r, k)
        y_send(f_blk, fy_s, fy_r.at.__getitem__, k)
        swap_send(0, k)

    add_chunks(0, 3)
    for k in Z_ORDER[:2]:
        pass_on(k)
    add_chunks(3, 4)
    for k in Z_ORDER[2:4]:
        pass_on(k)
    add_chunks(4, 5)
    for k in Z_ORDER[4:]:
        pass_on(k)
    add_chunks(5, 6)
    for k in FAR_FIRST:
        start(remote(w_blk(z, y), w_blk(z, y), wz_s, wz_r, at_z(zup[k])))
    arrived(wei.at[1, 0, pl.ds(0, 3)], wb_r)
    for k in FAR_FIRST:
        src = wei.at[1, z]
        start(remote(src, src, wc_s, wc_r, at_z(zup[k])))
    order = (0,) + Z_ORDER
    for k in order:
        arrived(fac.at[core, 0, pl.ds(0, 3)], fy_r.at[k])
        for d in (1, 3, 2):
            swap_send(d, k)
    arrived(fac.at[other], fd_r)

    for to in across:
        pl.semaphore_signal(met, inc=1, device_id=to, device_id_type=MESH)
    def factor(first, count):
        return jnp.concatenate(
            [fac[c, :, :, first:first + count, :].reshape(32 * count, 128) for c in (0, 1)], axis=1
        )

    low_q = dot(gq[...].astype(BF16), factor(0, 16)) * inv_root
    low_q = jnp.concatenate([low_q, jnp.zeros((256 - qcols, 256), F32)], axis=0).T
    low_o = (dot(go[...].astype(BF16), factor(16, 32)) * inv_root).T
    low_q, low_o = low_q.reshape(NZ, NY, 8, 256), low_o.reshape(NZ, NY, 8, 256)
    for lev in range(NZ):
        k = lax.rem(lev + NZ - z, NZ)
        upper = k // 4
        place = 2 * (k - 4) * (2 * upper - 1) - (1 - upper)
        for row in range(NY):
            part[row, place] = jnp.concatenate([low_q[lev, row], low_o[lev, row]], axis=0).astype(BF16)

    for i, (first, count) in enumerate(PIECES):
        piece = pl.ds(first, count)
        for d in (2, 1, 3):
            src = part.at[ups[d], piece]
            start(remote(src, part_in.at[d, piece], py_s, py_r.at[i], at_y(ups[d])))
    for i, (first, count) in enumerate(PIECES):
        piece = pl.ds(first, count)
        total = part[y, piece].astype(F32)
        arrived(part_in.at[pl.ds(1, 3), piece], py_r.at[i])
        for d in (3, 1, 2):
            total = total + part_in[d, piece].astype(F32)
        mid[piece] = total.astype(BF16)
        for j in range(first, first + count):
            k = BY_DISTANCE[j]
            if k:
                start(remote(mid.at[j], mid_in.at[k], pz_s, pz_r, at_z(zup[k])))
    pl.semaphore_wait(met, 3)
    arrived(wei.at[0, pl.ds(0, 7), 0], wz_r)
    for d in (2, 1, 3):
        src = wei.at[0, :, y]
        start(remote(src, src, wy_s, wy_r, at_y(ups[d])))
    arrived(mid_in.at[pl.ds(1, 7)], pz_r)
    low = mid[7].astype(F32)
    for k in Z_ORDER:
        low = low + mid_in[k].astype(F32)

    def moments(mean, square, low):
        mean_new = 0.8 * mean + 0.2 * low
        square_new = 0.9 * square + 0.1 * low * low
        return (mean_new, square_new, mean_new / jnp.sqrt(square_new))

    for copy in small[4:]:
        copy.wait()
    mq_v[...], sqq_v[...], dir_q = moments(qm_v[...], qs_v[...], low[0:8, 0:qcols])
    mo_v[...], soo_v[...], dir_o = moments(om_v[...], os_v[...], low[8:16, :])
    dir_q = jnp.concatenate([dir_q, jnp.zeros((8, 256 - qcols), F32)], axis=1)
    drc[z, y] = jnp.concatenate([dir_q, dir_o], axis=0).astype(BF16)
    z_send(d_blk, dz_s, dz_r)
    y_send(d_blk, dy_s, lambda k: dy_r, 0)

    sum_q = jnp.sum(dir_q * dir_q, axis=(0, 1), keepdims=True)
    sum_o = jnp.sum(dir_o * dir_o, axis=(0, 1), keepdims=True)
    sums[0] = jnp.concatenate([jnp.broadcast_to(sum_q, (1, 64)), jnp.broadcast_to(sum_o, (1, 64))], axis=1)
    for i, (d, e) in enumerate(SIDE):
        start(remote(sums.at[0], sums_in.at[i], sx_s, sx_r, side(d, e)))
    sent(fac.at[core, pl.ds(0, 7), 0], fz_s)
    sent(fac.at[core, pl.ds(0, 6)], fy_s)
    sent(fac.at[core], fd_s)
    sent(wei.at[1, 0, pl.ds(0, 3)], wb_s)
    sent(wei.at[0, pl.ds(0, 7), 0], wz_s)
    sent(part.at[pl.ds(0, 3)], py_s)
    sent(mid.at[pl.ds(0, 7)], pz_s)
    for k in Z_ORDER[:4]:
        z_wait(d_blk, dz_r, k)
        y_send(d_blk, dy_s, lambda k: dy_r, k)
    for k in Z_ORDER[4:]:
        z_wait(d_blk, dz_r, k)
        y_send(d_blk, dy_s, lambda k: dy_r, k)
    arrived(sums_in.at[pl.ds(0, 31)], sx_r)
    total = sums[0] + jnp.sum(sums_in[0:31], axis=0)
    sums[1] = total

    def sum_copies():
        return [
            remote(sums.at[1], sums_in.at[31 + k], sz_s, sz_r, (zup[k] * NY + y, tp - c))
            for k in FAR_FIRST
            for c in (1, 0)
        ]

    @pl.when(core == 1)
    def _():
        for copy in sum_copies():
            copy.start()

    arrived(drc.at[pl.ds(0, 6)], dy_r)
    every = drc[...].astype(F32).reshape(32, 16, 256)
    pq[...] = dot(factor(0, 16), every[:, 0:8].reshape(256, 256).astype(BF16))
    po[...] = dot(factor(16, 32), every[:, 8:16].reshape(256, 256).astype(BF16))
    arrived(sums_in.at[pl.ds(32, 7)], sz_r)
    total = total + jnp.sum(sums_in[32:39], axis=0)
    count = 256.0 * 8 * qcols
    scale_q = lax.rsqrt(total[0:1, 0:1] / count + 0.25)
    scale_o = lax.rsqrt(total[0:1, 64:65] / (256.0 * 8 * 256) + 0.25)

    own_q = pq[pl.ds(pl.multiple_of(fs * 16, 16), 16), :][:, 0:qcols] * scale_q
    own_o = po[pl.ds(pl.multiple_of(fs * 32, 32), 32), :] * scale_o
    sq_v[...] = own_q
    so_v[...] = own_o
    nq_v[...] = qw_v[...] - 0.02 * own_q
    no_v[...] = ow_v[...] - 0.02 * own_o
    arrived(wei.at[0, :, pl.ds(0, 3)], wy_r)
    arrived(wei.at[1, pl.ds(0, 7)], wc_r)
    weights = jnp.concatenate([wei[0].reshape(32, 48, 128), wei[1].reshape(32, 48, 128)], axis=2).astype(F32)
    weights_q = weights[:, 0:16].reshape(512, 256)
    weights_o = weights[:, 16:48].reshape(1024, 256)
    cq[...] = (weights_q - 0.02 * (pq[...] * scale_q)).T[0:qcols, :].astype(BF16)
    co[...] = (weights_o - 0.02 * (po[...] * scale_o)).astype(BF16)
    sent(wei.at[1, pl.ds(0, 7)], wc_s)
    sent(wei.at[0, :, pl.ds(0, 3)], wy_s)
    sent(drc.at[pl.ds(0, 7), 0], dz_s)
    sent(drc.at[pl.ds(0, 6)], dy_s)
    sent(sums_in.at[pl.ds(0, 31)], sx_s)

    @pl.when(core == 1)
    def _():
        sent(sums_in.at[pl.ds(0, 14)], sz_s)


def write_out(*refs):
    n = len(refs) // 2
    sem = refs[-1]
    copies = [pltpu.make_async_copy(refs[i], refs[n + i], sem.at[i]) for i in range(n)]
    for copy in copies:
        copy.start()
    for copy in copies:
        copy.wait()


def solution(mesh):
    def on_device(lat, qcot, att, mix, qw, ow, qf, of, qm, qs, om, os_):
        tokens, qcols = lat.shape[0], qw.shape[1]
        inv_root = 1.0 / math.sqrt(tokens * lax.axis_size("fs"))

        def like(a):
            return jax.ShapeDtypeStruct(a.shape, a.dtype)

        def vm(a):
            return pltpu.VMEM(a.shape, a.dtype)

        dma = pltpu.SemaphoreType.DMA
        any_ = pl.BlockSpec(memory_space=pl.ANY)
        outs = (
            like(qw), like(ow), like(qw), like(ow),
            jax.ShapeDtypeStruct((qcols, 512), BF16), jax.ShapeDtypeStruct((1024, 256), BF16),
            like(qm), like(qs), like(om), like(os_),
        )
        qcot = qcot.T
        held = pl.pallas_call(
            functools.partial(kernel, inv_root),
            out_shape=[pltpu.VMEM(a.shape, a.dtype) for a in outs],
            in_specs=[any_] * 12,
            out_specs=[pl.BlockSpec(memory_space=pltpu.VMEM)] * 10,
            scratch_shapes=[
                vm(lat), vm(qcot), vm(att), vm(mix), vm(qw), vm(ow), vm(qm), vm(qs), vm(om), vm(os_),
                pltpu.VMEM((qcols, 512), F32), pltpu.VMEM((256, 1024), F32),
                pltpu.VMEM((2, NZ, NY, 48, 128), BF16), pltpu.VMEM((2, NZ, NY, 48, 128), BF16),
                pltpu.VMEM((NY, NZ, 16, 256), BF16), pltpu.VMEM((NY, NZ, 16, 256), BF16),
                pltpu.VMEM((NZ, 16, 256), BF16), pltpu.VMEM((NZ, 16, 256), BF16),
                pltpu.VMEM((NZ, NY, 16, 256), BF16),
                pltpu.VMEM((2, 1, 128), F32), pltpu.VMEM((39, 1, 128), F32),
                pltpu.VMEM((512, 256), F32), pltpu.VMEM((1024, 256), F32),
                dma((CHUNKS, 4)), dma((8,)),
                dma, dma((8,)), dma, dma((8,)), dma, dma,
                dma, dma, dma, dma, dma, dma, dma, dma,
                dma, dma((4,)), dma, dma,
                dma, dma((8,)), dma, dma,
                dma, dma, dma, dma, pltpu.SemaphoreType.REGULAR,
            ],
            compiler_params=pltpu.CompilerParams(
                collective_id=0, has_side_effects=True, vmem_limit_bytes=56 * 1024 * 1024
            ),
        )(lat, qcot, att, mix, qw, ow, qf, of, qm, qs, om, os_)
        results = pl.pallas_call(
            write_out,
            out_shape=outs,
            in_specs=[pl.BlockSpec(memory_space=pltpu.VMEM)] * 10,
            out_specs=[any_] * 10,
            scratch_shapes=[dma((10,))],
        )(*[pltpu.with_memory_space_constraint(a, pltpu.VMEM) for a in held])
        return (*results[:4], results[4].T, *results[5:])

    rows, both, whole = P("fs", None), P("fs", "tp"), P(None, "tp")
    return jax.shard_map(
        on_device,
        mesh=mesh,
        in_specs=(rows, both, rows, both, both, both, rows, rows, both, both, both, both),
        out_specs=(both, both, both, both, whole, whole, both, both, both, both),
        check_vma=False,
    )
```

```python
import functools
import math

import jax
import jax.numpy as jnp
from jax import lax
from jax.experimental import pallas as pl
from jax.experimental.pallas import tpu as pltpu
from jax.sharding import PartitionSpec as P

MESH = pl.DeviceIdType.MESH
F32 = jnp.float32
BF16 = jnp.bfloat16
NZ, NY = 8, 4
CHUNKS = 6
Z_ORDER = (1, 7, 2, 6, 3, 5, 4)
GROUPS = ((1, 7), (2, 6), (3, 5), (4,))
GROUP_OF = {k: i for i, ks in enumerate(GROUPS) for k in ks}
FAR_FIRST = (4, 3, 5, 2, 6, 1, 7)
BY_DISTANCE = (4, 3, 5, 2, 6, 1, 7, 0)
PIECES = ((0, 1), (1, 2), (3, 2), (5, 3))
SIDE = [(d, e) for d in range(NY) for e in range(8) if d or e]


def by_tokens(left, right):
    return lax.dot_general(left, right, (((0,), (0,)), ((), ())), preferred_element_type=F32)


def dot(left, right):
    return jnp.dot(left, right, preferred_element_type=F32)


def kernel(
    inv_root,
    lat, qcot, att, mix, qw, ow, qf, of, qm, qs, om, os_,
    sq_v, so_v, nq_v, no_v, pq, po, wei, scales, mq_v, sqq_v, mo_v, soo_v,
    rows_v, qcot_v, qw_v, ow_v, mq_in, mo_in,
    gq, go, gqb, gob, fac, part, part_in, mid, mid_in, drc, sums, sums_in,
    chunk_sem, small_sem,
    fz_s, fz_r, fy_s, fy_r, fd_s, fd_r,
    wz_s, wz_r, wy_s, wy_r, wb_s, wb_r, wc_s, wc_r,
    py_s, py_r, pz_s, pz_r,
    dz_s, dz_r, dy_s, dy_r,
    sx_s, sx_r, sz_s, sz_r, met,
):
    fs, tp = lax.axis_index("fs"), lax.axis_index("tp")
    y, z = lax.rem(fs, NY), fs // NY
    core = lax.rem(tp, 2)
    other = 1 - core
    partner = (fs, tp + 1 - 2 * core)
    ups = [lax.rem(y + d, NY) for d in range(NY)]
    downs = [lax.rem(y + NY - d, NY) for d in range(NY)]
    zup = [lax.rem(z + d, NZ) for d in range(NZ)]
    zdn = [lax.rem(z + NZ - d, NZ) for d in range(NZ)]

    def at_y(row):
        return (z * NY + row, tp)

    def at_z(level):
        return (level * NY + y, tp)

    def side(d, e):
        return (z * NY + ups[d], lax.rem(tp + e, 8))

    def remote(src, dst, send, recv, to):
        return pltpu.make_async_remote_copy(
            src_ref=src, dst_ref=dst, send_sem=send, recv_sem=recv, device_id=to, device_id_type=MESH
        )

    def arrived(ref, sem):
        pltpu.make_async_copy(ref, ref, sem).wait()

    sent = arrived
    half = pl.ds(pl.multiple_of(core * 128, 128), 128)
    own = fac.at[core, z, y]
    for src, dst, i in (
        (qf.at[:, half], own.at[pl.ds(0, 16)], 0),
        (of.at[:, half], own.at[pl.ds(16, 32)], 0),
        (qw, qw_v, 1), (ow, ow_v, 2),
        (qm, mq_in.at[0], 3), (qs, mq_in.at[1], 3), (om, mo_in.at[0], 4), (os_, mo_in.at[1], 4),
    ):
        pltpu.make_async_copy(src, dst, small_sem.at[i]).start()

    across = [(fs, lax.rem(tp + e, 8)) for e in (4, 2, 6)]
    barrier = pltpu.get_barrier_semaphore()
    for to in [at_z(zup[k]) for k in FAR_FIRST] + [at_y(ups[d]) for d in (2, 1, 3)] + [partner] + across:
        pl.semaphore_signal(barrier, inc=1, device_id=to, device_id_type=MESH)

    tokens = lat.shape[0]
    rows = tokens // CHUNKS
    pairs = ((lat, pl.ds(0, 512)), (mix, pl.ds(512, 256)), (att, pl.ds(768, 1024)))

    def chunk_copies(i):
        span = pl.ds(pl.multiple_of(i * rows, rows), rows)
        copies = [
            pltpu.make_async_copy(src.at[span], rows_v.at[span, columns], chunk_sem.at[i, 0])
            for src, columns in pairs
        ]
        copies.append(pltpu.make_async_copy(qcot.at[:, span], qcot_v.at[:, span], chunk_sem.at[i, 1]))
        return copies

    def add_chunk(i):
        span = pl.ds(pl.multiple_of(i * rows, rows), rows)
        arrived(rows_v.at[span], chunk_sem.at[i, 0])
        arrived(qcot_v.at[:, span], chunk_sem.at[i, 1])
        gq[...] += dot(qcot_v[:, span], rows_v[span, 0:512])
        go[...] += by_tokens(rows_v[span, 512:768], rows_v[span, 768:1792])

    def add_chunks(a, b):
        @pl.loop(a, b)
        def _(i):
            add_chunk(i)

    for i, ref in enumerate((own, qw_v, ow_v)):
        arrived(ref, small_sem.at[i])
    for i in range(CHUNKS):
        for copy in chunk_copies(i):
            copy.start()
    qcols = qw_v.shape[1]
    wei[0, z, y, 0:16] = qw_v[:, 0:128].astype(BF16)
    wei[1, z, y, 0:16, 0:qcols - 128] = qw_v[:, 128:qcols].astype(BF16)
    for i in (0, 1):
        wei[i, z, y, 16:48] = ow_v[:, 128 * i:128 * i + 128].astype(BF16)

    pl.semaphore_wait(barrier, 14)

    def f_blk(level, row):
        return fac.at[core, level, row]

    def w_blk(level, row):
        return wei.at[0, level, row]

    def d_blk(level, row):
        return drc.at[level, row]

    def start(copy):
        copy.start()

    def z_send(blk, s, r):
        for k in FAR_FIRST:
            start(remote(blk(z, y), blk(z, y), s, r.at[GROUP_OF[k]], at_z(zup[k])))

    def y_send(blk, s, r, k):
        for d in (2, 1, 3):
            start(remote(blk(zdn[k], y), blk(zdn[k], y), s, r(k), at_y(ups[d])))

    def swap_send(d, k):
        src = f_blk(zdn[k], downs[d])
        start(remote(src, src, fd_s, fd_r, partner))

    z_send(f_blk, fz_s, fz_r)
    y_send(f_blk, fy_s, lambda k: fy_r.at[4], 0)
    swap_send(0, 0)
    for d in (2, 1, 3):
        src = wei.at[1, z, y]
        start(remote(src, src, wb_s, wb_r, at_y(ups[d])))
    gq[...] = jnp.zeros_like(gq)
    go[...] = jnp.zeros_like(go)

    def pass_on(g):
        arrived(fac.at[core, pl.ds(0, len(GROUPS[g])), 0], fz_r.at[g])
        for k in GROUPS[g]:
            y_send(f_blk, fy_s, lambda k: fy_r.at[GROUP_OF[k]], k)
            swap_send(0, k)

    add_chunks(0, 3)
    pass_on(0)
    add_chunks(3, 4)
    pass_on(1)
    add_chunks(4, 5)
    pass_on(2)
    pass_on(3)
    add_chunks(5, 6)
    for k in FAR_FIRST:
        start(remote(w_blk(z, y), w_blk(z, y), wz_s, wz_r, at_z(zup[k])))
    arrived(wei.at[1, 0, pl.ds(0, 3)], wb_r)
    for k in FAR_FIRST:
        src = wei.at[1, z]
        start(remote(src, src, wc_s, wc_r, at_z(zup[k])))
    gqb[...] = gq[...].astype(BF16)
    gob[...] = go[...].astype(BF16)
    for g, ks in ((4, (0,)), *enumerate(GROUPS)):
        arrived(fac.at[core, pl.ds(0, len(ks)), pl.ds(0, 3)], fy_r.at[g])
        for k in ks:
            for d in (1, 3, 2):
                swap_send(d, k)
    arrived(fac.at[other], fd_r)

    for to in across:
        pl.semaphore_signal(met, inc=1, device_id=to, device_id_type=MESH)
    def factor(first, count):
        return jnp.concatenate(
            [fac[c, :, :, first:first + count, :].reshape(32 * count, 128) for c in (0, 1)], axis=1
        )

    low_q = dot(gqb[...], factor(0, 16)) * inv_root
    low_q = jnp.concatenate([low_q, jnp.zeros((256 - qcols, 256), F32)], axis=0).T
    low_o = (dot(gob[...], factor(16, 32)) * inv_root).T
    low_q, low_o = low_q.reshape(NZ, NY, 8, 256), low_o.reshape(NZ, NY, 8, 256)
    for lev in range(NZ):
        k = lax.rem(lev + NZ - z, NZ)
        upper = k // 4
        place = 2 * (k - 4) * (2 * upper - 1) - (1 - upper)
        for row in range(NY):
            part[row, place] = jnp.concatenate([low_q[lev, row], low_o[lev, row]], axis=0).astype(BF16)

    for i, (first, count) in enumerate(PIECES):
        piece = pl.ds(first, count)
        for d in (2, 1, 3):
            src = part.at[ups[d], piece]
            start(remote(src, part_in.at[d, piece], py_s, py_r.at[i], at_y(ups[d])))
    for i, (first, count) in enumerate(PIECES):
        piece = pl.ds(first, count)
        total = part[y, piece].astype(F32)
        arrived(part_in.at[pl.ds(1, 3), piece], py_r.at[i])
        for d in (3, 1, 2):
            total = total + part_in[d, piece].astype(F32)
        mid[piece] = total.astype(BF16)
        for j in range(first, first + count):
            k = BY_DISTANCE[j]
            if k:
                start(remote(mid.at[j], mid_in.at[k], pz_s, pz_r, at_z(zup[k])))
    pl.semaphore_wait(met, 3)
    arrived(wei.at[0, pl.ds(0, 7), 0], wz_r)
    for d in (2, 1, 3):
        src = wei.at[0, :, y]
        start(remote(src, src, wy_s, wy_r, at_y(ups[d])))
    arrived(mid_in.at[pl.ds(1, 7)], pz_r)
    low = mid[7].astype(F32)
    for k in Z_ORDER:
        low = low + mid_in[k].astype(F32)

    def moments(mean, square, low):
        mean_new = 0.8 * mean + 0.2 * low
        square_new = 0.9 * square + 0.1 * low * low
        return (mean_new, square_new, mean_new / jnp.sqrt(square_new))

    arrived(mq_in, small_sem.at[3])
    arrived(mo_in, small_sem.at[4])
    mq_v[...], sqq_v[...], dir_q = moments(mq_in[0], mq_in[1], low[0:8, 0:qcols])
    mo_v[...], soo_v[...], dir_o = moments(mo_in[0], mo_in[1], low[8:16, :])
    dir_q = jnp.concatenate([dir_q, jnp.zeros((8, 256 - qcols), F32)], axis=1)
    drc[z, y] = jnp.concatenate([dir_q, dir_o], axis=0).astype(BF16)
    z_send(d_blk, dz_s, dz_r)
    y_send(d_blk, dy_s, lambda k: dy_r, 0)

    sum_q = jnp.sum(dir_q * dir_q, axis=(0, 1), keepdims=True)
    sum_o = jnp.sum(dir_o * dir_o, axis=(0, 1), keepdims=True)
    sums[0] = jnp.concatenate([jnp.broadcast_to(sum_q, (1, 64)), jnp.broadcast_to(sum_o, (1, 64))], axis=1)
    for i, (d, e) in enumerate(SIDE):
        start(remote(sums.at[0], sums_in.at[i], sx_s, sx_r, side(d, e)))
    sent(fac.at[core, pl.ds(0, 7), 0], fz_s)
    sent(fac.at[core, pl.ds(0, 6)], fy_s)
    sent(fac.at[core], fd_s)
    sent(wei.at[1, 0, pl.ds(0, 3)], wb_s)
    sent(wei.at[0, pl.ds(0, 7), 0], wz_s)
    sent(part.at[pl.ds(0, 3)], py_s)
    sent(mid.at[pl.ds(0, 7)], pz_s)
    for g, ks in enumerate(GROUPS):
        arrived(drc.at[pl.ds(0, len(ks)), 0], dz_r.at[g])
        for k in ks:
            y_send(d_blk, dy_s, lambda k: dy_r, k)
    arrived(sums_in.at[pl.ds(0, 31)], sx_r)
    total = sums[0] + jnp.sum(sums_in[0:31], axis=0)
    sums[1] = total

    def sum_copies():
        return [
            remote(sums.at[1], sums_in.at[31 + k], sz_s, sz_r, (zup[k] * NY + y, tp - c))
            for k in FAR_FIRST
            for c in (1, 0)
        ]

    @pl.when(core == 1)
    def _():
        for copy in sum_copies():
            copy.start()

    arrived(drc.at[pl.ds(0, 6)], dy_r)
    every = drc[...].astype(F32).reshape(32, 16, 256)
    pq[...] = dot(factor(0, 16), every[:, 0:8].reshape(256, 256).astype(BF16))
    po[...] = dot(factor(16, 32), every[:, 8:16].reshape(256, 256).astype(BF16))
    arrived(wei.at[0, :, pl.ds(0, 3)], wy_r)
    arrived(wei.at[1, pl.ds(0, 7)], wc_r)
    sent(wei.at[1, pl.ds(0, 7)], wc_s)
    sent(wei.at[0, :, pl.ds(0, 3)], wy_s)
    sent(drc.at[pl.ds(0, 7), 0], dz_s)
    sent(drc.at[pl.ds(0, 6)], dy_s)
    sent(sums_in.at[pl.ds(0, 31)], sx_s)

    @pl.when(core == 1)
    def _():
        sent(sums_in.at[pl.ds(0, 14)], sz_s)

    arrived(sums_in.at[pl.ds(32, 7)], sz_r)
    total = total + jnp.sum(sums_in[32:39], axis=0)
    count = 256.0 * 8 * qcols
    scale_q = lax.rsqrt(total[0:1, 0:1] / count + 0.25)
    scale_o = lax.rsqrt(total[0:1, 64:65] / (256.0 * 8 * 256) + 0.25)

    scales[...] = jnp.concatenate([jnp.broadcast_to(scale_q, (1, 64)), jnp.broadcast_to(scale_o, (1, 64))], axis=1)
    own_q = pq[pl.ds(pl.multiple_of(fs * 16, 16), 16), :][:, 0:qcols] * scale_q
    own_o = po[pl.ds(pl.multiple_of(fs * 32, 32), 32), :] * scale_o
    sq_v[...] = own_q
    so_v[...] = own_o
    nq_v[...] = qw_v[...] - 0.02 * own_q
    no_v[...] = ow_v[...] - 0.02 * own_o


def write_out(
    sq_v, so_v, nq_v, no_v, pq, po, wei, scales, mq_v, sqq_v, mo_v, soo_v,
    step_q, step_o, new_q, new_o, copy_q, copy_o, mean_q, square_q, mean_o, square_o,
    cq, co, sem,
):
    copies = []

    def put(src, dst):
        copies.append(pltpu.make_async_copy(src, dst, sem.at[len(copies)]))
        copies[-1].start()

    for src, dst in (
        (sq_v, step_q), (so_v, step_o), (nq_v, new_q), (no_v, new_o),
        (mq_v, mean_q), (sqq_v, square_q), (mo_v, mean_o), (soo_v, square_o),
    ):
        put(src, dst)
    scale_q, scale_o = scales[0:1, 0:1], scales[0:1, 64:65]

    def weights(levels, rows):
        halves = [wei[i, levels, :, rows, :] for i in (0, 1)]
        both = jnp.concatenate([h.reshape(-1, 128) for h in halves], axis=1)
        return both.astype(F32)

    for j in range(4):
        span = pl.ds(256 * j, 256)
        old = weights(slice(2 * j, 2 * j + 2), slice(16, 48))
        co[span, :] = (old - 0.02 * (po[span, :] * scale_o)).astype(BF16)
        put(co.at[span], copy_o.at[span])
        if j == 1:
            old = weights(slice(0, NZ), slice(0, 16))
            cq[...] = (old - 0.02 * (pq[...] * scale_q)).T[0:cq.shape[0], :].astype(BF16)
            put(cq, copy_q)
    for copy in copies:
        copy.wait()


def solution(mesh):
    def on_device(lat, qcot, att, mix, qw, ow, qf, of, qm, qs, om, os_):
        tokens, qcols = lat.shape[0], qw.shape[1]
        inv_root = 1.0 / math.sqrt(tokens * lax.axis_size("fs"))

        def like(a):
            return jax.ShapeDtypeStruct(a.shape, a.dtype)

        def vm(a):
            return pltpu.VMEM(a.shape, a.dtype)

        dma = pltpu.SemaphoreType.DMA
        any_ = pl.BlockSpec(memory_space=pl.ANY)
        outs = (
            like(qw), like(ow), like(qw), like(ow),
            jax.ShapeDtypeStruct((qcols, 512), BF16), jax.ShapeDtypeStruct((1024, 256), BF16),
            like(qm), like(qs), like(om), like(os_),
        )
        kept = [vm(qw), vm(ow), vm(qw), vm(ow)]
        kept += [pltpu.VMEM((512, 256), F32), pltpu.VMEM((1024, 256), F32)]
        kept += [pltpu.VMEM((2, NZ, NY, 48, 128), BF16), pltpu.VMEM((1, 128), F32)]
        kept += [vm(qm), vm(qs), vm(om), vm(os_)]
        qcot = qcot.T
        held = pl.pallas_call(
            functools.partial(kernel, inv_root),
            out_shape=kept,
            in_specs=[any_] * 12,
            out_specs=[pl.BlockSpec(memory_space=pltpu.VMEM)] * 12,
            scratch_shapes=[
                pltpu.VMEM((tokens, 1792), BF16), vm(qcot), vm(qw), vm(ow),
                pltpu.VMEM((2, 8, qcols), F32), pltpu.VMEM((2, 8, 256), F32),
                pltpu.VMEM((qcols, 512), F32), pltpu.VMEM((256, 1024), F32),
                pltpu.VMEM((qcols, 512), BF16), pltpu.VMEM((256, 1024), BF16),
                pltpu.VMEM((2, NZ, NY, 48, 128), BF16),
                pltpu.VMEM((NY, NZ, 16, 256), BF16), pltpu.VMEM((NY, NZ, 16, 256), BF16),
                pltpu.VMEM((NZ, 16, 256), BF16), pltpu.VMEM((NZ, 16, 256), BF16),
                pltpu.VMEM((NZ, NY, 16, 256), BF16),
                pltpu.VMEM((2, 1, 128), F32), pltpu.VMEM((39, 1, 128), F32),
                dma((CHUNKS, 2)), dma((5,)),
                dma, dma((4,)), dma, dma((5,)), dma, dma,
                dma, dma, dma, dma, dma, dma, dma, dma,
                dma, dma((4,)), dma, dma,
                dma, dma((4,)), dma, dma,
                dma, dma, dma, dma, pltpu.SemaphoreType.REGULAR,
            ],
            compiler_params=pltpu.CompilerParams(
                collective_id=0, has_side_effects=True, vmem_limit_bytes=56 * 1024 * 1024
            ),
        )(lat, qcot, att, mix, qw, ow, qf, of, qm, qs, om, os_)
        results = pl.pallas_call(
            write_out,
            out_shape=outs,
            in_specs=[pl.BlockSpec(memory_space=pltpu.VMEM)] * 12,
            out_specs=[any_] * 10,
            scratch_shapes=[pltpu.VMEM((qcols, 512), BF16), pltpu.VMEM((1024, 256), BF16), dma((13,))],
        )(*[pltpu.with_memory_space_constraint(a, pltpu.VMEM) for a in held])
        return (*results[:4], results[4].T, *results[5:])

    rows, both, whole = P("fs", None), P("fs", "tp"), P(None, "tp")
    return jax.shard_map(
        on_device,
        mesh=mesh,
        in_specs=(rows, both, rows, both, both, both, rows, rows, both, both, both, both),
        out_specs=(both, both, both, both, whole, whole, both, both, both, both),
        check_vma=False,
    )
```

```python
import functools
import math

import jax
import jax.numpy as jnp
from jax import lax
from jax.experimental import pallas as pl
from jax.experimental.pallas import tpu as pltpu
from jax.sharding import PartitionSpec as P

MESH = pl.DeviceIdType.MESH
F32 = jnp.float32
BF16 = jnp.bfloat16
NZ, NY = 8, 4
CHUNKS = 6
Z_ORDER = (1, 7, 2, 6, 3, 5, 4)
GROUPS = ((1, 7), (2, 6), (3, 5), (4,))
GROUP_OF = {k: i for i, ks in enumerate(GROUPS) for k in ks}
FAR_FIRST = (4, 3, 5, 2, 6, 1, 7)
BY_DISTANCE = (4, 3, 5, 2, 6, 1, 7, 0)
PIECES = ((0, 1), (1, 2), (3, 2), (5, 3))
SIDE = [(d, e) for d in range(NY) for e in range(8) if d or e]


def by_tokens(left, right):
    return lax.dot_general(left, right, (((0,), (0,)), ((), ())), preferred_element_type=F32)


def dot(left, right):
    return jnp.dot(left, right, preferred_element_type=F32)


def kernel(
    inv_root,
    lat, qcot, att, mix, qw, ow, qf, of, qm, qs, om, os_,
    sq_v, so_v, nq_v, no_v, pq, po, wei, scales, mq_v, sqq_v, mo_v, soo_v,
    rows_v, qcot_v, qw_v, ow_v, mq_in, mo_in,
    gq, go, gqb, gob, fac, part, part_in, mid, mid_in, drc, sums, sums_in,
    chunk_sem, small_sem,
    fz_s, fz_r, fy_s, fy_r, fd_s, fd_r,
    wz_s, wz_r, wy_s, wy_r, wb_s, wb_r, wc_s, wc_r,
    py_s, py_r, pz_s, pz_r,
    dz_s, dz_r, dy_s, dy_r,
    sx_s, sx_r, sz_s, sz_r, met,
):
    fs, tp = lax.axis_index("fs"), lax.axis_index("tp")
    y, z = lax.rem(fs, NY), fs // NY
    core = lax.rem(tp, 2)
    other = 1 - core
    partner = (fs, tp + 1 - 2 * core)
    ups = [lax.rem(y + d, NY) for d in range(NY)]
    downs = [lax.rem(y + NY - d, NY) for d in range(NY)]
    zup = [lax.rem(z + d, NZ) for d in range(NZ)]
    zdn = [lax.rem(z + NZ - d, NZ) for d in range(NZ)]

    def at_y(row):
        return (z * NY + row, tp)

    def at_z(level):
        return (level * NY + y, tp)

    def side(d, e):
        return (z * NY + ups[d], lax.rem(tp + e, 8))

    def remote(src, dst, send, recv, to):
        return pltpu.make_async_remote_copy(
            src_ref=src, dst_ref=dst, send_sem=send, recv_sem=recv, device_id=to, device_id_type=MESH
        )

    def arrived(ref, sem):
        pltpu.make_async_copy(ref, ref, sem).wait()

    sent = arrived
    half = pl.ds(pl.multiple_of(core * 128, 128), 128)
    own = fac.at[core, z, y]
    for src, dst, i in (
        (qf.at[:, half], own.at[pl.ds(0, 16)], 0),
        (of.at[:, half], own.at[pl.ds(16, 32)], 0),
        (qw, qw_v, 1), (ow, ow_v, 2),
        (qm, mq_in.at[0], 3), (qs, mq_in.at[1], 3), (om, mo_in.at[0], 4), (os_, mo_in.at[1], 4),
    ):
        pltpu.make_async_copy(src, dst, small_sem.at[i]).start()

    across = [(fs, lax.rem(tp + e, 8)) for e in (4, 2, 6)]
    barrier = pltpu.get_barrier_semaphore()
    for to in [at_z(zup[k]) for k in FAR_FIRST] + [at_y(ups[d]) for d in (2, 1, 3)] + [partner] + across:
        pl.semaphore_signal(barrier, inc=1, device_id=to, device_id_type=MESH)

    tokens = lat.shape[0]
    rows = tokens // CHUNKS
    pairs = ((lat, pl.ds(0, 512)), (mix, pl.ds(512, 256)), (att, pl.ds(768, 1024)))

    def chunk_copies(i):
        span = pl.ds(pl.multiple_of(i * rows, rows), rows)
        copies = [
            pltpu.make_async_copy(src.at[span], rows_v.at[span, columns], chunk_sem.at[i, 0])
            for src, columns in pairs
        ]
        copies.append(pltpu.make_async_copy(qcot.at[:, span], qcot_v.at[:, span], chunk_sem.at[i, 1]))
        return copies

    def add_chunk(i):
        span = pl.ds(pl.multiple_of(i * rows, rows), rows)
        arrived(rows_v.at[span], chunk_sem.at[i, 0])
        arrived(qcot_v.at[:, span], chunk_sem.at[i, 1])
        gq[...] += dot(qcot_v[:, span], rows_v[span, 0:512])
        go[...] += by_tokens(rows_v[span, 512:768], rows_v[span, 768:1792])

    def add_chunks(a, b):
        @pl.loop(a, b)
        def _(i):
            add_chunk(i)

    for i, ref in enumerate((own, qw_v, ow_v)):
        arrived(ref, small_sem.at[i])
    for i in range(CHUNKS):
        for copy in chunk_copies(i):
            copy.start()
    qcols = qw_v.shape[1]
    wei[z, y, 0:16, 0:qcols] = qw_v[...].astype(BF16)
    wei[z, y, 16:48] = ow_v[...].astype(BF16)

    pl.semaphore_wait(barrier, 14)

    def f_blk(level, row):
        return fac.at[core, level, row]

    q_rows, o_rows = pl.ds(0, 16), pl.ds(16, 32)

    def w_blk(level, row):
        return wei.at[level, row, o_rows]

    def d_blk(level, row):
        return drc.at[level, row]

    def start(copy):
        copy.start()

    def z_send(blk, s, r):
        for k in FAR_FIRST:
            start(remote(blk(z, y), blk(z, y), s, r.at[GROUP_OF[k]], at_z(zup[k])))

    def y_send(blk, s, r, k):
        for d in (2, 1, 3):
            start(remote(blk(zdn[k], y), blk(zdn[k], y), s, r(k), at_y(ups[d])))

    def swap_send(d, k):
        src = f_blk(zdn[k], downs[d])
        start(remote(src, src, fd_s, fd_r, partner))

    z_send(f_blk, fz_s, fz_r)
    y_send(f_blk, fy_s, lambda k: fy_r.at[4], 0)
    swap_send(0, 0)
    for d in (2, 1, 3):
        src = wei.at[z, y, q_rows]
        start(remote(src, src, wb_s, wb_r, at_y(ups[d])))
    gq[...] = jnp.zeros_like(gq)
    go[...] = jnp.zeros_like(go)

    def pass_on(g):
        arrived(fac.at[core, pl.ds(0, len(GROUPS[g])), 0], fz_r.at[g])
        for k in GROUPS[g]:
            y_send(f_blk, fy_s, lambda k: fy_r.at[GROUP_OF[k]], k)
            swap_send(0, k)

    add_chunks(0, 3)
    pass_on(0)
    add_chunks(3, 4)
    pass_on(1)
    add_chunks(4, 5)
    pass_on(2)
    pass_on(3)
    add_chunks(5, 6)
    for k in FAR_FIRST:
        start(remote(w_blk(z, y), w_blk(z, y), wz_s, wz_r, at_z(zup[k])))
    arrived(wei.at[0, pl.ds(0, 3), q_rows], wb_r)
    for k in FAR_FIRST:
        src = wei.at[z, :, q_rows]
        start(remote(src, src, wc_s, wc_r, at_z(zup[k])))
    gqb[...] = gq[...].astype(BF16)
    gob[...] = go[...].astype(BF16)
    for g, ks in ((4, (0,)), *enumerate(GROUPS)):
        arrived(fac.at[core, pl.ds(0, len(ks)), pl.ds(0, 3)], fy_r.at[g])
        for k in ks:
            for d in (1, 3, 2):
                swap_send(d, k)
    arrived(fac.at[other], fd_r)

    for to in across:
        pl.semaphore_signal(met, inc=1, device_id=to, device_id_type=MESH)
    def factor(first, count):
        return jnp.concatenate(
            [fac[c, :, :, first:first + count, :].reshape(32 * count, 128) for c in (0, 1)], axis=1
        )

    low_q = dot(gqb[...], factor(0, 16)) * inv_root
    low_q = jnp.concatenate([low_q, jnp.zeros((256 - qcols, 256), F32)], axis=0).T
    low_o = (dot(gob[...], factor(16, 32)) * inv_root).T
    low_q, low_o = low_q.reshape(NZ, NY, 8, 256), low_o.reshape(NZ, NY, 8, 256)
    for lev in range(NZ):
        k = lax.rem(lev + NZ - z, NZ)
        upper = k // 4
        place = 2 * (k - 4) * (2 * upper - 1) - (1 - upper)
        for row in range(NY):
            part[row, place] = jnp.concatenate([low_q[lev, row], low_o[lev, row]], axis=0).astype(BF16)

    for i, (first, count) in enumerate(PIECES):
        piece = pl.ds(first, count)
        for d in (2, 1, 3):
            src = part.at[ups[d], piece]
            start(remote(src, part_in.at[d, piece], py_s, py_r.at[i], at_y(ups[d])))
    for i, (first, count) in enumerate(PIECES):
        piece = pl.ds(first, count)
        total = part[y, piece].astype(F32)
        arrived(part_in.at[pl.ds(1, 3), piece], py_r.at[i])
        for d in (3, 1, 2):
            total = total + part_in[d, piece].astype(F32)
        mid[piece] = total.astype(BF16)
        for j in range(first, first + count):
            k = BY_DISTANCE[j]
            if k:
                start(remote(mid.at[j], mid_in.at[k], pz_s, pz_r, at_z(zup[k])))
    pl.semaphore_wait(met, 3)
    arrived(wei.at[pl.ds(0, 7), 0, o_rows], wz_r)
    for d in (2, 1, 3):
        src = wei.at[:, y, o_rows]
        start(remote(src, src, wy_s, wy_r, at_y(ups[d])))
    arrived(mid_in.at[pl.ds(1, 7)], pz_r)
    low = mid[7].astype(F32)
    for k in Z_ORDER:
        low = low + mid_in[k].astype(F32)

    def moments(mean, square, low):
        mean_new = 0.8 * mean + 0.2 * low
        square_new = 0.9 * square + 0.1 * low * low
        return (mean_new, square_new, mean_new / jnp.sqrt(square_new))

    arrived(mq_in, small_sem.at[3])
    arrived(mo_in, small_sem.at[4])
    mq_v[...], sqq_v[...], dir_q = moments(mq_in[0], mq_in[1], low[0:8, 0:qcols])
    mo_v[...], soo_v[...], dir_o = moments(mo_in[0], mo_in[1], low[8:16, :])
    dir_q = jnp.concatenate([dir_q, jnp.zeros((8, 256 - qcols), F32)], axis=1)
    drc[z, y] = jnp.concatenate([dir_q, dir_o], axis=0).astype(BF16)
    sum_q = jnp.sum(dir_q * dir_q, axis=(0, 1), keepdims=True)
    sum_o = jnp.sum(dir_o * dir_o, axis=(0, 1), keepdims=True)
    sums[0] = jnp.concatenate([jnp.broadcast_to(sum_q, (1, 64)), jnp.broadcast_to(sum_o, (1, 64))], axis=1)
    for i, (d, e) in enumerate(SIDE):
        start(remote(sums.at[0], sums_in.at[i], sx_s, sx_r, side(d, e)))
    z_send(d_blk, dz_s, dz_r)
    y_send(d_blk, dy_s, lambda k: dy_r, 0)

    sent(fac.at[core, pl.ds(0, 7), 0], fz_s)
    sent(fac.at[core, pl.ds(0, 6)], fy_s)
    sent(fac.at[core], fd_s)
    sent(wei.at[0, pl.ds(0, 3), q_rows], wb_s)
    sent(wei.at[pl.ds(0, 7), 0, o_rows], wz_s)
    sent(part.at[pl.ds(0, 3)], py_s)
    sent(mid.at[pl.ds(0, 7)], pz_s)
    for g, ks in enumerate(GROUPS):
        arrived(drc.at[pl.ds(0, len(ks)), 0], dz_r.at[g])
        for k in ks:
            y_send(d_blk, dy_s, lambda k: dy_r, k)
    arrived(sums_in.at[pl.ds(0, 31)], sx_r)
    total = sums[0] + jnp.sum(sums_in[0:31], axis=0)
    sums[1] = total

    def sum_copies():
        return [
            remote(sums.at[1], sums_in.at[31 + k], sz_s, sz_r, (zup[k] * NY + y, tp - c))
            for k in FAR_FIRST
            for c in (1, 0)
        ]

    @pl.when(core == 1)
    def _():
        for copy in sum_copies():
            copy.start()

    arrived(drc.at[pl.ds(0, 6)], dy_r)
    every = drc[...].astype(F32).reshape(32, 16, 256)
    pq[...] = dot(factor(0, 16), every[:, 0:8].reshape(256, 256).astype(BF16))
    po[...] = dot(factor(16, 32), every[:, 8:16].reshape(256, 256).astype(BF16))
    arrived(wei.at[:, pl.ds(0, 3), o_rows], wy_r)
    arrived(wei.at[pl.ds(0, 7), :, q_rows], wc_r)
    sent(wei.at[pl.ds(0, 7), :, q_rows], wc_s)
    sent(wei.at[:, pl.ds(0, 3), o_rows], wy_s)
    sent(drc.at[pl.ds(0, 7), 0], dz_s)
    sent(drc.at[pl.ds(0, 6)], dy_s)
    sent(sums_in.at[pl.ds(0, 31)], sx_s)

    @pl.when(core == 1)
    def _():
        sent(sums_in.at[pl.ds(0, 14)], sz_s)

    arrived(sums_in.at[pl.ds(32, 7)], sz_r)
    total = total + jnp.sum(sums_in[32:39], axis=0)
    count = 256.0 * 8 * qcols
    scale_q = lax.rsqrt(total[0:1, 0:1] / count + 0.25)
    scale_o = lax.rsqrt(total[0:1, 64:65] / (256.0 * 8 * 256) + 0.25)

    scales[...] = jnp.concatenate([jnp.broadcast_to(scale_q, (1, 64)), jnp.broadcast_to(scale_o, (1, 64))], axis=1)
    own_q = pq[pl.ds(pl.multiple_of(fs * 16, 16), 16), :][:, 0:qcols] * scale_q
    own_o = po[pl.ds(pl.multiple_of(fs * 32, 32), 32), :] * scale_o
    sq_v[...] = own_q
    so_v[...] = own_o
    nq_v[...] = qw_v[...] - 0.02 * own_q
    no_v[...] = ow_v[...] - 0.02 * own_o


def write_out(
    sq_v, so_v, nq_v, no_v, pq, po, wei, scales, mq_v, sqq_v, mo_v, soo_v,
    step_q, step_o, new_q, new_o, copy_q, copy_o, mean_q, square_q, mean_o, square_o,
    cq, co, sem,
):
    copies = []

    def put(src, dst):
        copies.append(pltpu.make_async_copy(src, dst, sem.at[len(copies)]))
        copies[-1].start()

    for src, dst in (
        (sq_v, step_q), (so_v, step_o), (nq_v, new_q), (no_v, new_o),
        (mq_v, mean_q), (sqq_v, square_q), (mo_v, mean_o), (soo_v, square_o),
    ):
        put(src, dst)
    scale_q, scale_o = scales[0:1, 0:1], scales[0:1, 64:65]

    def weights(levels, rows):
        return wei[levels, :, rows, :].reshape(-1, 256).astype(F32)

    for j in range(4):
        span = pl.ds(256 * j, 256)
        old = weights(slice(2 * j, 2 * j + 2), slice(16, 48))
        co[span, :] = (old - 0.02 * (po[span, :] * scale_o)).astype(BF16)
        put(co.at[span], copy_o.at[span])
        if j == 1:
            old = weights(slice(0, NZ), slice(0, 16))
            cq[...] = (old - 0.02 * (pq[...] * scale_q)).T[0:cq.shape[0], :].astype(BF16)
            put(cq, copy_q)
    for copy in copies:
        copy.wait()


def solution(mesh):
    def on_device(lat, qcot, att, mix, qw, ow, qf, of, qm, qs, om, os_):
        tokens, qcols = lat.shape[0], qw.shape[1]
        inv_root = 1.0 / math.sqrt(tokens * lax.axis_size("fs"))

        def like(a):
            return jax.ShapeDtypeStruct(a.shape, a.dtype)

        def vm(a):
            return pltpu.VMEM(a.shape, a.dtype)

        dma = pltpu.SemaphoreType.DMA
        any_ = pl.BlockSpec(memory_space=pl.ANY)
        outs = (
            like(qw), like(ow), like(qw), like(ow),
            jax.ShapeDtypeStruct((qcols, 512), BF16), jax.ShapeDtypeStruct((1024, 256), BF16),
            like(qm), like(qs), like(om), like(os_),
        )
        kept = [vm(qw), vm(ow), vm(qw), vm(ow)]
        kept += [pltpu.VMEM((512, 256), F32), pltpu.VMEM((1024, 256), F32)]
        kept += [pltpu.VMEM((NZ, NY, 48, 256), BF16), pltpu.VMEM((1, 128), F32)]
        kept += [vm(qm), vm(qs), vm(om), vm(os_)]
        qcot = qcot.T
        held = pl.pallas_call(
            functools.partial(kernel, inv_root),
            out_shape=kept,
            in_specs=[any_] * 12,
            out_specs=[pl.BlockSpec(memory_space=pltpu.VMEM)] * 12,
            scratch_shapes=[
                pltpu.VMEM((tokens, 1792), BF16), vm(qcot), vm(qw), vm(ow),
                pltpu.VMEM((2, 8, qcols), F32), pltpu.VMEM((2, 8, 256), F32),
                pltpu.VMEM((qcols, 512), F32), pltpu.VMEM((256, 1024), F32),
                pltpu.VMEM((qcols, 512), BF16), pltpu.VMEM((256, 1024), BF16),
                pltpu.VMEM((2, NZ, NY, 48, 128), BF16),
                pltpu.VMEM((NY, NZ, 16, 256), BF16), pltpu.VMEM((NY, NZ, 16, 256), BF16),
                pltpu.VMEM((NZ, 16, 256), BF16), pltpu.VMEM((NZ, 16, 256), BF16),
                pltpu.VMEM((NZ, NY, 16, 256), BF16),
                pltpu.VMEM((2, 1, 128), F32), pltpu.VMEM((39, 1, 128), F32),
                dma((CHUNKS, 2)), dma((5,)),
                dma, dma((4,)), dma, dma((5,)), dma, dma,
                dma, dma, dma, dma, dma, dma, dma, dma,
                dma, dma((4,)), dma, dma,
                dma, dma((4,)), dma, dma,
                dma, dma, dma, dma, pltpu.SemaphoreType.REGULAR,
            ],
            compiler_params=pltpu.CompilerParams(
                collective_id=0, has_side_effects=True, vmem_limit_bytes=56 * 1024 * 1024
            ),
        )(lat, qcot, att, mix, qw, ow, qf, of, qm, qs, om, os_)
        results = pl.pallas_call(
            write_out,
            out_shape=outs,
            in_specs=[pl.BlockSpec(memory_space=pltpu.VMEM)] * 12,
            out_specs=[any_] * 10,
            scratch_shapes=[pltpu.VMEM((qcols, 512), BF16), pltpu.VMEM((1024, 256), BF16), dma((13,))],
        )(*[pltpu.with_memory_space_constraint(a, pltpu.VMEM) for a in held])
        return (*results[:4], results[4].T, *results[5:])

    rows, both, whole = P("fs", None), P("fs", "tp"), P(None, "tp")
    return jax.shard_map(
        on_device,
        mesh=mesh,
        in_specs=(rows, both, rows, both, both, both, rows, rows, both, both, both, both),
        out_specs=(both, both, both, both, whole, whole, both, both, both, both),
        check_vma=False,
    )
```

```python
import functools
import math

import jax
import jax.numpy as jnp
from jax import lax
from jax.experimental import pallas as pl
from jax.experimental.pallas import tpu as pltpu
from jax.sharding import PartitionSpec as P

MESH = pl.DeviceIdType.MESH
F32 = jnp.float32
BF16 = jnp.bfloat16
NZ, NY = 8, 4
CHUNKS = 6
Z_ORDER = (1, 7, 2, 6, 3, 5, 4)
GROUPS = ((1, 7), (2, 6), (3, 5), (4,))
GROUP_OF = {k: i for i, ks in enumerate(GROUPS) for k in ks}
FAR_FIRST = (4, 3, 5, 2, 6, 1, 7)
BY_DISTANCE = (4, 3, 5, 2, 6, 1, 7, 0)
PIECES = ((0, 1), (1, 2), (3, 2), (5, 3))
SIDE = [(d, e) for d in range(NY) for e in range(8) if d or e]


def by_tokens(left, right):
    return lax.dot_general(left, right, (((0,), (0,)), ((), ())), preferred_element_type=F32)


def dot(left, right):
    return jnp.dot(left, right, preferred_element_type=F32)


def kernel(
    inv_root,
    lat, qcot, att, mix, qw, ow, qf, of, qm, qs, om, os_,
    sq_v, so_v, nq_v, no_v, pq, po, wei, scales, mq_v, sqq_v, mo_v, soo_v,
    rows_v, qcot_v, qw_v, ow_v, mq_in, mo_in,
    gq, go, gqb, gob, fac, part, part_in, mid, mid_in, drc, sums, sums_in,
    chunk_sem, small_sem,
    fz_s, fz_r, fy_s, fy_r, fd_s, fd_r,
    wz_s, wz_r, wy_s, wy_r, wb_s, wb_r, wc_s, wc_r,
    py_s, py_r, pz_s, pz_r,
    dz_s, dz_r, dy_s, dy_r,
    sx_s, sx_r, sz_s, sz_r, met,
):
    fs, tp = lax.axis_index("fs"), lax.axis_index("tp")
    y, z = lax.rem(fs, NY), fs // NY
    core = lax.rem(tp, 2)
    other = 1 - core
    partner = (fs, tp + 1 - 2 * core)
    ups = [lax.rem(y + d, NY) for d in range(NY)]
    downs = [lax.rem(y + NY - d, NY) for d in range(NY)]
    zup = [lax.rem(z + d, NZ) for d in range(NZ)]
    zdn = [lax.rem(z + NZ - d, NZ) for d in range(NZ)]

    def at_y(row):
        return (z * NY + row, tp)

    def at_z(level):
        return (level * NY + y, tp)

    def side(d, e):
        return (z * NY + ups[d], lax.rem(tp + e, 8))

    def remote(src, dst, send, recv, to):
        return pltpu.make_async_remote_copy(
            src_ref=src, dst_ref=dst, send_sem=send, recv_sem=recv, device_id=to, device_id_type=MESH
        )

    def arrived(ref, sem):
        pltpu.make_async_copy(ref, ref, sem).wait()

    sent = arrived
    half = pl.ds(pl.multiple_of(core * 128, 128), 128)
    own = fac.at[core, z, y]
    for src, dst, i in (
        (qf.at[:, half], own.at[pl.ds(0, 16)], 0),
        (of.at[:, half], own.at[pl.ds(16, 32)], 0),
        (qw, qw_v, 1), (ow, ow_v, 2),
        (qm, mq_in.at[0], 3), (qs, mq_in.at[1], 3), (om, mo_in.at[0], 4), (os_, mo_in.at[1], 4),
    ):
        pltpu.make_async_copy(src, dst, small_sem.at[i]).start()

    across = [(fs, lax.rem(tp + e, 8)) for e in (4, 2, 6)]
    barrier = pltpu.get_barrier_semaphore()
    for to in [at_z(zup[k]) for k in FAR_FIRST] + [at_y(ups[d]) for d in (2, 1, 3)] + [partner] + across:
        pl.semaphore_signal(barrier, inc=1, device_id=to, device_id_type=MESH)

    tokens = lat.shape[0]
    rows = tokens // CHUNKS
    pairs = ((lat, pl.ds(0, 512)), (mix, pl.ds(512, 256)), (att, pl.ds(768, 1024)))

    def chunk_copies(i):
        span = pl.ds(pl.multiple_of(i * rows, rows), rows)
        copies = [
            pltpu.make_async_copy(src.at[span], rows_v.at[span, columns], chunk_sem.at[i, 0])
            for src, columns in pairs
        ]
        copies.append(pltpu.make_async_copy(qcot.at[:, span], qcot_v.at[:, span], chunk_sem.at[i, 1]))
        return copies

    def add_chunk(i):
        span = pl.ds(pl.multiple_of(i * rows, rows), rows)
        arrived(rows_v.at[span], chunk_sem.at[i, 0])
        arrived(qcot_v.at[:, span], chunk_sem.at[i, 1])
        gq[...] += dot(qcot_v[:, span], rows_v[span, 0:512])
        go[...] += by_tokens(rows_v[span, 512:768], rows_v[span, 768:1792])

    def add_chunks(a, b):
        @pl.loop(a, b)
        def _(i):
            add_chunk(i)

    for i, ref in enumerate((own, qw_v, ow_v)):
        arrived(ref, small_sem.at[i])
    for i in range(CHUNKS):
        for copy in chunk_copies(i):
            copy.start()
    qcols = qw_v.shape[1]
    wei[z, y, 0:16, 0:qcols] = qw_v[...].astype(BF16)
    wei[z, y, 16:48] = ow_v[...].astype(BF16)

    pl.semaphore_wait(barrier, 14)

    def f_blk(level, row):
        return fac.at[core, level, row]

    q_rows, o_rows = pl.ds(0, 16), pl.ds(16, 32)

    def w_blk(level, row):
        return wei.at[level, row, o_rows]

    def d_blk(level, row):
        return drc.at[level, row]

    def start(copy):
        copy.start()

    def z_send(blk, s, r):
        for k in FAR_FIRST:
            start(remote(blk(z, y), blk(z, y), s, r.at[GROUP_OF[k]], at_z(zup[k])))

    def y_send(blk, s, r, k):
        for d in (2, 1, 3):
            start(remote(blk(zdn[k], y), blk(zdn[k], y), s, r(k), at_y(ups[d])))

    def swap_send(d, k):
        src = f_blk(zdn[k], downs[d])
        start(remote(src, src, fd_s, fd_r, partner))

    z_send(f_blk, fz_s, fz_r)
    y_send(f_blk, fy_s, lambda k: fy_r.at[4], 0)
    swap_send(0, 0)
    for d in (2, 1, 3):
        src = wei.at[z, y, q_rows]
        start(remote(src, src, wb_s, wb_r, at_y(ups[d])))
    gq[...] = jnp.zeros_like(gq)
    go[...] = jnp.zeros_like(go)

    def pass_on(g):
        arrived(fac.at[core, pl.ds(0, len(GROUPS[g])), 0], fz_r.at[g])
        for k in GROUPS[g]:
            y_send(f_blk, fy_s, lambda k: fy_r.at[GROUP_OF[k]], k)
            swap_send(0, k)

    add_chunks(0, 3)
    pass_on(0)
    add_chunks(3, 4)
    pass_on(1)
    add_chunks(4, 5)
    pass_on(2)
    pass_on(3)
    add_chunks(5, 6)
    for k in FAR_FIRST:
        start(remote(w_blk(z, y), w_blk(z, y), wz_s, wz_r, at_z(zup[k])))
    arrived(wei.at[0, pl.ds(0, 3), q_rows], wb_r)
    for k in FAR_FIRST:
        src = wei.at[z, :, q_rows]
        start(remote(src, src, wc_s, wc_r, at_z(zup[k])))
    gqb[...] = gq[...].astype(BF16)
    gob[...] = go[...].astype(BF16)
    for g, ks in ((4, (0,)), *enumerate(GROUPS)):
        arrived(fac.at[core, pl.ds(0, len(ks)), pl.ds(0, 3)], fy_r.at[g])
        for k in ks:
            for d in (1, 3, 2):
                swap_send(d, k)
    arrived(fac.at[other], fd_r)

    for to in across:
        pl.semaphore_signal(met, inc=1, device_id=to, device_id_type=MESH)
    def factor(first, count):
        return jnp.concatenate(
            [fac[c, :, :, first:first + count, :].reshape(32 * count, 128) for c in (0, 1)], axis=1
        )

    low_q = dot(gqb[...], factor(0, 16)) * inv_root
    low_q = jnp.concatenate([low_q, jnp.zeros((256 - qcols, 256), F32)], axis=0).T
    low_o = (dot(gob[...], factor(16, 32)) * inv_root).T
    low_q, low_o = low_q.reshape(NZ, NY, 8, 256), low_o.reshape(NZ, NY, 8, 256)
    for lev in range(NZ):
        k = lax.rem(lev + NZ - z, NZ)
        upper = k // 4
        place = 2 * (k - 4) * (2 * upper - 1) - (1 - upper)
        for row in range(NY):
            part[row, place] = jnp.concatenate([low_q[lev, row], low_o[lev, row]], axis=0).astype(BF16)

    for i, (first, count) in enumerate(PIECES):
        piece = pl.ds(first, count)
        for d in (2, 1, 3):
            src = part.at[ups[d], piece]
            start(remote(src, part_in.at[d, piece], py_s, py_r.at[i], at_y(ups[d])))
    for i, (first, count) in enumerate(PIECES):
        piece = pl.ds(first, count)
        total = part[y, piece].astype(F32)
        arrived(part_in.at[pl.ds(1, 3), piece], py_r.at[i])
        for d in (3, 1, 2):
            total = total + part_in[d, piece].astype(F32)
        mid[piece] = total.astype(BF16)
        for j in range(first, first + count):
            k = BY_DISTANCE[j]
            if k:
                start(remote(mid.at[j], mid_in.at[k], pz_s, pz_r, at_z(zup[k])))
        if i == 2:
            arrived(wei.at[pl.ds(0, 7), 0, o_rows], wz_r)
            for d in (2, 1, 3):
                src = wei.at[:, y, o_rows]
                start(remote(src, src, wy_s, wy_r, at_y(ups[d])))
    pl.semaphore_wait(met, 3)
    arrived(mid_in.at[pl.ds(1, 7)], pz_r)
    low = mid[7].astype(F32)
    for k in Z_ORDER:
        low = low + mid_in[k].astype(F32)

    def moments(mean, square, low):
        mean_new = 0.8 * mean + 0.2 * low
        square_new = 0.9 * square + 0.1 * low * low
        return (mean_new, square_new, mean_new / jnp.sqrt(square_new))

    arrived(mq_in, small_sem.at[3])
    arrived(mo_in, small_sem.at[4])
    mq_v[...], sqq_v[...], dir_q = moments(mq_in[0], mq_in[1], low[0:8, 0:qcols])
    mo_v[...], soo_v[...], dir_o = moments(mo_in[0], mo_in[1], low[8:16, :])
    dir_q = jnp.concatenate([dir_q, jnp.zeros((8, 256 - qcols), F32)], axis=1)
    drc[z, y] = jnp.concatenate([dir_q, dir_o], axis=0).astype(BF16)
    sum_q = jnp.sum(dir_q * dir_q, axis=(0, 1), keepdims=True)
    sum_o = jnp.sum(dir_o * dir_o, axis=(0, 1), keepdims=True)
    sums[0] = jnp.concatenate([jnp.broadcast_to(sum_q, (1, 64)), jnp.broadcast_to(sum_o, (1, 64))], axis=1)
    for i, (d, e) in enumerate(SIDE):
        start(remote(sums.at[0], sums_in.at[i], sx_s, sx_r, side(d, e)))
    z_send(d_blk, dz_s, dz_r)
    y_send(d_blk, dy_s, lambda k: dy_r, 0)

    sent(fac.at[core, pl.ds(0, 7), 0], fz_s)
    sent(fac.at[core, pl.ds(0, 6)], fy_s)
    sent(fac.at[core], fd_s)
    sent(wei.at[0, pl.ds(0, 3), q_rows], wb_s)
    sent(wei.at[pl.ds(0, 7), 0, o_rows], wz_s)
    sent(part.at[pl.ds(0, 3)], py_s)
    sent(mid.at[pl.ds(0, 7)], pz_s)
    for g, ks in enumerate(GROUPS):
        arrived(drc.at[pl.ds(0, len(ks)), 0], dz_r.at[g])
        for k in ks:
            y_send(d_blk, dy_s, lambda k: dy_r, k)
    arrived(sums_in.at[pl.ds(0, 31)], sx_r)
    total = sums[0] + jnp.sum(sums_in[0:31], axis=0)
    sums[1] = total

    def sum_copies():
        return [
            remote(sums.at[1], sums_in.at[31 + k], sz_s, sz_r, (zup[k] * NY + y, tp - c))
            for k in FAR_FIRST
            for c in (1, 0)
        ]

    @pl.when(core == 1)
    def _():
        for copy in sum_copies():
            copy.start()

    arrived(drc.at[pl.ds(0, 6)], dy_r)
    every = drc[...].astype(F32).reshape(32, 16, 256)
    pq[...] = dot(factor(0, 16), every[:, 0:8].reshape(256, 256).astype(BF16))
    po[...] = dot(factor(16, 32), every[:, 8:16].reshape(256, 256).astype(BF16))
    arrived(wei.at[:, pl.ds(0, 3), o_rows], wy_r)
    arrived(wei.at[pl.ds(0, 7), :, q_rows], wc_r)
    sent(wei.at[pl.ds(0, 7), :, q_rows], wc_s)
    sent(wei.at[:, pl.ds(0, 3), o_rows], wy_s)
    sent(drc.at[pl.ds(0, 7), 0], dz_s)
    sent(drc.at[pl.ds(0, 6)], dy_s)
    sent(sums_in.at[pl.ds(0, 31)], sx_s)

    @pl.when(core == 1)
    def _():
        sent(sums_in.at[pl.ds(0, 14)], sz_s)

    arrived(sums_in.at[pl.ds(32, 7)], sz_r)
    total = total + jnp.sum(sums_in[32:39], axis=0)
    count = 256.0 * 8 * qcols
    scale_q = lax.rsqrt(total[0:1, 0:1] / count + 0.25)
    scale_o = lax.rsqrt(total[0:1, 64:65] / (256.0 * 8 * 256) + 0.25)

    scales[...] = jnp.concatenate([jnp.broadcast_to(scale_q, (1, 64)), jnp.broadcast_to(scale_o, (1, 64))], axis=1)
    own_q = pq[pl.ds(pl.multiple_of(fs * 16, 16), 16), :][:, 0:qcols] * scale_q
    own_o = po[pl.ds(pl.multiple_of(fs * 32, 32), 32), :] * scale_o
    sq_v[...] = own_q
    so_v[...] = own_o
    nq_v[...] = qw_v[...] - 0.02 * own_q
    no_v[...] = ow_v[...] - 0.02 * own_o


def write_out(
    sq_v, so_v, nq_v, no_v, pq, po, wei, scales, mq_v, sqq_v, mo_v, soo_v,
    step_q, step_o, new_q, new_o, copy_q, copy_o, mean_q, square_q, mean_o, square_o,
    cq, co, sem,
):
    copies = []

    def put(src, dst):
        copies.append(pltpu.make_async_copy(src, dst, sem.at[len(copies)]))
        copies[-1].start()

    for src, dst in (
        (sq_v, step_q), (so_v, step_o), (nq_v, new_q), (no_v, new_o),
        (mq_v, mean_q), (sqq_v, square_q), (mo_v, mean_o), (soo_v, square_o),
    ):
        put(src, dst)
    scale_q, scale_o = scales[0:1, 0:1], scales[0:1, 64:65]

    def weights(levels, rows):
        return wei[levels, :, rows, :].reshape(-1, 256).astype(F32)

    for j in range(4):
        span = pl.ds(256 * j, 256)
        old = weights(slice(2 * j, 2 * j + 2), slice(16, 48))
        co[span, :] = (old - 0.02 * (po[span, :] * scale_o)).astype(BF16)
        put(co.at[span], copy_o.at[span])
        if j == 1:
            old = weights(slice(0, NZ), slice(0, 16))
            cq[...] = (old - 0.02 * (pq[...] * scale_q)).T[0:cq.shape[0], :].astype(BF16)
            put(cq, copy_q)
    for copy in copies:
        copy.wait()


def solution(mesh):
    def on_device(lat, qcot, att, mix, qw, ow, qf, of, qm, qs, om, os_):
        tokens, qcols = lat.shape[0], qw.shape[1]
        inv_root = 1.0 / math.sqrt(tokens * lax.axis_size("fs"))

        def like(a):
            return jax.ShapeDtypeStruct(a.shape, a.dtype)

        def vm(a):
            return pltpu.VMEM(a.shape, a.dtype)

        dma = pltpu.SemaphoreType.DMA
        any_ = pl.BlockSpec(memory_space=pl.ANY)
        outs = (
            like(qw), like(ow), like(qw), like(ow),
            jax.ShapeDtypeStruct((qcols, 512), BF16), jax.ShapeDtypeStruct((1024, 256), BF16),
            like(qm), like(qs), like(om), like(os_),
        )
        kept = [vm(qw), vm(ow), vm(qw), vm(ow)]
        kept += [pltpu.VMEM((512, 256), F32), pltpu.VMEM((1024, 256), F32)]
        kept += [pltpu.VMEM((NZ, NY, 48, 256), BF16), pltpu.VMEM((1, 128), F32)]
        kept += [vm(qm), vm(qs), vm(om), vm(os_)]
        qcot = qcot.T
        held = pl.pallas_call(
            functools.partial(kernel, inv_root),
            out_shape=kept,
            in_specs=[any_] * 12,
            out_specs=[pl.BlockSpec(memory_space=pltpu.VMEM)] * 12,
            scratch_shapes=[
                pltpu.VMEM((tokens, 1792), BF16), vm(qcot), vm(qw), vm(ow),
                pltpu.VMEM((2, 8, qcols), F32), pltpu.VMEM((2, 8, 256), F32),
                pltpu.VMEM((qcols, 512), F32), pltpu.VMEM((256, 1024), F32),
                pltpu.VMEM((qcols, 512), BF16), pltpu.VMEM((256, 1024), BF16),
                pltpu.VMEM((2, NZ, NY, 48, 128), BF16),
                pltpu.VMEM((NY, NZ, 16, 256), BF16), pltpu.VMEM((NY, NZ, 16, 256), BF16),
                pltpu.VMEM((NZ, 16, 256), BF16), pltpu.VMEM((NZ, 16, 256), BF16),
                pltpu.VMEM((NZ, NY, 16, 256), BF16),
                pltpu.VMEM((2, 1, 128), F32), pltpu.VMEM((39, 1, 128), F32),
                dma((CHUNKS, 2)), dma((5,)),
                dma, dma((4,)), dma, dma((5,)), dma, dma,
                dma, dma, dma, dma, dma, dma, dma, dma,
                dma, dma((4,)), dma, dma,
                dma, dma((4,)), dma, dma,
                dma, dma, dma, dma, pltpu.SemaphoreType.REGULAR,
            ],
            compiler_params=pltpu.CompilerParams(
                collective_id=0, has_side_effects=True, vmem_limit_bytes=56 * 1024 * 1024
            ),
        )(lat, qcot, att, mix, qw, ow, qf, of, qm, qs, om, os_)
        results = pl.pallas_call(
            write_out,
            out_shape=outs,
            in_specs=[pl.BlockSpec(memory_space=pltpu.VMEM)] * 12,
            out_specs=[any_] * 10,
            scratch_shapes=[pltpu.VMEM((qcols, 512), BF16), pltpu.VMEM((1024, 256), BF16), dma((13,))],
        )(*[pltpu.with_memory_space_constraint(a, pltpu.VMEM) for a in held])
        return (*results[:4], results[4].T, *results[5:])

    rows, both, whole = P("fs", None), P("fs", "tp"), P(None, "tp")
    return jax.shard_map(
        on_device,
        mesh=mesh,
        in_specs=(rows, both, rows, both, both, both, rows, rows, both, both, both, both),
        out_specs=(both, both, both, both, whole, whole, both, both, both, both),
        check_vma=False,
    )
```

```python
import functools
import math

import jax
import jax.numpy as jnp
from jax import lax
from jax.experimental import pallas as pl
from jax.experimental.pallas import tpu as pltpu
from jax.sharding import PartitionSpec as P

MESH = pl.DeviceIdType.MESH
F32 = jnp.float32
BF16 = jnp.bfloat16
NZ, NY = 8, 4
CHUNKS = 6
Z_ORDER = (1, 7, 2, 6, 3, 5, 4)
GROUPS = ((1, 7), (2, 6), (3, 5), (4,))
GROUP_OF = {k: i for i, ks in enumerate(GROUPS) for k in ks}
FAR_FIRST = (4, 3, 5, 2, 6, 1, 7)
BY_DISTANCE = (4, 3, 5, 2, 6, 1, 7, 0)
PIECES = ((0, 1), (1, 2), (3, 2), (5, 3))
SIDE = [(d, e) for d in range(NY) for e in range(8) if d or e]


def by_tokens(left, right):
    return lax.dot_general(left, right, (((0,), (0,)), ((), ())), preferred_element_type=F32)


def dot(left, right):
    return jnp.dot(left, right, preferred_element_type=F32)


def kernel(
    inv_root,
    lat, qcot, att, mix, qw, ow, qf, of, qm, qs, om, os_,
    sq_v, so_v, nq_v, no_v, pq, po, wei, scales, mq_v, sqq_v, mo_v, soo_v,
    rows_v, qcot_v, qw_v, ow_v, mq_in, mo_in,
    gq, go, gqb, gob, fac, part, part_in, mid, mid_in, drc, sums, sums_in,
    chunk_sem, small_sem,
    fz_s, fz_r, fy_s, fy_r, fd_s, fd_r,
    wz_s, wz_r, wy_s, wy_r, wb_s, wb_r, wc_s, wc_r,
    py_s, py_r, pz_s, pz_r,
    dz_s, dz_r, dy_s, dy_r,
    sx_s, sx_r, sz_s, sz_r, met,
):
    fs, tp = lax.axis_index("fs"), lax.axis_index("tp")
    y, z = lax.rem(fs, NY), fs // NY
    core = lax.rem(tp, 2)
    other = 1 - core
    partner = (fs, tp + 1 - 2 * core)
    ups = [lax.rem(y + d, NY) for d in range(NY)]
    downs = [lax.rem(y + NY - d, NY) for d in range(NY)]
    zup = [lax.rem(z + d, NZ) for d in range(NZ)]
    zdn = [lax.rem(z + NZ - d, NZ) for d in range(NZ)]

    def at_y(row):
        return (z * NY + row, tp)

    def at_z(level):
        return (level * NY + y, tp)

    def side(d, e):
        return (z * NY + ups[d], lax.rem(tp + e, 8))

    def remote(src, dst, send, recv, to):
        return pltpu.make_async_remote_copy(
            src_ref=src, dst_ref=dst, send_sem=send, recv_sem=recv, device_id=to, device_id_type=MESH
        )

    def arrived(ref, sem):
        pltpu.make_async_copy(ref, ref, sem).wait()

    sent = arrived
    half = pl.ds(pl.multiple_of(core * 128, 128), 128)
    own = fac.at[core, z, y]
    for src, dst, i in (
        (qf.at[:, half], own.at[pl.ds(0, 16)], 0),
        (of.at[:, half], own.at[pl.ds(16, 32)], 0),
        (qw, qw_v, 1), (ow, ow_v, 2),
        (qm, mq_in.at[0], 3), (qs, mq_in.at[1], 3), (om, mo_in.at[0], 4), (os_, mo_in.at[1], 4),
    ):
        pltpu.make_async_copy(src, dst, small_sem.at[i]).start()

    across = [(fs, lax.rem(tp + e, 8)) for e in (4, 2, 6)]
    barrier = pltpu.get_barrier_semaphore()
    for to in [at_z(zup[k]) for k in FAR_FIRST] + [at_y(ups[d]) for d in (2, 1, 3)] + [partner] + across:
        pl.semaphore_signal(barrier, inc=1, device_id=to, device_id_type=MESH)

    tokens = lat.shape[0]
    rows = tokens // CHUNKS
    pairs = ((lat, pl.ds(0, 512)), (mix, pl.ds(512, 256)), (att, pl.ds(768, 1024)))

    def chunk_copies(i):
        span = pl.ds(pl.multiple_of(i * rows, rows), rows)
        copies = [
            pltpu.make_async_copy(src.at[span], rows_v.at[span, columns], chunk_sem.at[i, 0])
            for src, columns in pairs
        ]
        copies.append(pltpu.make_async_copy(qcot.at[:, span], qcot_v.at[:, span], chunk_sem.at[i, 1]))
        return copies

    def add_chunk(i):
        span = pl.ds(pl.multiple_of(i * rows, rows), rows)
        arrived(rows_v.at[span], chunk_sem.at[i, 0])
        arrived(qcot_v.at[:, span], chunk_sem.at[i, 1])
        gq[...] += dot(qcot_v[:, span], rows_v[span, 0:512])
        go[...] += by_tokens(rows_v[span, 512:768], rows_v[span, 768:1792])

    def add_chunks(a, b):
        @pl.loop(a, b)
        def _(i):
            add_chunk(i)

    for i, ref in enumerate((own, qw_v, ow_v)):
        arrived(ref, small_sem.at[i])
    for i in range(CHUNKS):
        for copy in chunk_copies(i):
            copy.start()
    qcols = qw_v.shape[1]
    wei[z, y, 0:16, 0:qcols] = qw_v[...].astype(BF16)
    wei[z, y, 16:48] = ow_v[...].astype(BF16)

    pl.semaphore_wait(barrier, 14)

    def f_blk(level, row):
        return fac.at[core, level, row]

    q_rows, o_rows = pl.ds(0, 16), pl.ds(16, 32)

    def w_blk(level, row):
        return wei.at[level, row, o_rows]

    def d_blk(level, row):
        return drc.at[level, row]

    def start(copy):
        copy.start()

    def z_send(blk, s, r):
        for k in FAR_FIRST:
            start(remote(blk(z, y), blk(z, y), s, r.at[GROUP_OF[k]], at_z(zup[k])))

    def y_send(blk, s, r, k):
        for d in (2, 1, 3):
            start(remote(blk(zdn[k], y), blk(zdn[k], y), s, r(k), at_y(ups[d])))

    def swap_send(d, k):
        src = f_blk(zdn[k], downs[d])
        start(remote(src, src, fd_s, fd_r, partner))

    z_send(f_blk, fz_s, fz_r)
    y_send(f_blk, fy_s, lambda k: fy_r.at[4], 0)
    swap_send(0, 0)
    for d in (2, 1, 3):
        src = wei.at[z, y, q_rows]
        start(remote(src, src, wb_s, wb_r, at_y(ups[d])))
    gq[...] = jnp.zeros_like(gq)
    go[...] = jnp.zeros_like(go)

    def pass_on(g):
        arrived(fac.at[core, pl.ds(0, len(GROUPS[g])), 0], fz_r.at[g])
        for k in GROUPS[g]:
            y_send(f_blk, fy_s, lambda k: fy_r.at[GROUP_OF[k]], k)
            swap_send(0, k)

    add_chunks(0, 5)
    for g in range(len(GROUPS)):
        pass_on(g)
    add_chunks(5, 6)
    for k in FAR_FIRST:
        start(remote(w_blk(z, y), w_blk(z, y), wz_s, wz_r, at_z(zup[k])))
    arrived(wei.at[0, pl.ds(0, 3), q_rows], wb_r)
    for k in FAR_FIRST:
        src = wei.at[z, :, q_rows]
        start(remote(src, src, wc_s, wc_r, at_z(zup[k])))
    gqb[...] = gq[...].astype(BF16)
    gob[...] = go[...].astype(BF16)
    for g, ks in ((4, (0,)), *enumerate(GROUPS)):
        arrived(fac.at[core, pl.ds(0, len(ks)), pl.ds(0, 3)], fy_r.at[g])
        for k in ks:
            for d in (1, 3, 2):
                swap_send(d, k)
    arrived(fac.at[other], fd_r)

    for to in across:
        pl.semaphore_signal(met, inc=1, device_id=to, device_id_type=MESH)
    def factor(first, count):
        return jnp.concatenate(
            [fac[c, :, :, first:first + count, :].reshape(32 * count, 128) for c in (0, 1)], axis=1
        )

    low_q = dot(gqb[...], factor(0, 16)) * inv_root
    low_q = jnp.concatenate([low_q, jnp.zeros((256 - qcols, 256), F32)], axis=0).T
    low_o = (dot(gob[...], factor(16, 32)) * inv_root).T
    low_q, low_o = low_q.reshape(NZ, NY, 8, 256), low_o.reshape(NZ, NY, 8, 256)
    for lev in range(NZ):
        k = lax.rem(lev + NZ - z, NZ)
        upper = k // 4
        place = 2 * (k - 4) * (2 * upper - 1) - (1 - upper)
        for row in range(NY):
            part[row, place] = jnp.concatenate([low_q[lev, row], low_o[lev, row]], axis=0).astype(BF16)

    for i, (first, count) in enumerate(PIECES):
        piece = pl.ds(first, count)
        for d in (2, 1, 3):
            src = part.at[ups[d], piece]
            start(remote(src, part_in.at[d, piece], py_s, py_r.at[i], at_y(ups[d])))
    for i, (first, count) in enumerate(PIECES):
        piece = pl.ds(first, count)
        total = part[y, piece].astype(F32)
        arrived(part_in.at[pl.ds(1, 3), piece], py_r.at[i])
        for d in (3, 1, 2):
            total = total + part_in[d, piece].astype(F32)
        mid[piece] = total.astype(BF16)
        for j in range(first, first + count):
            k = BY_DISTANCE[j]
            if k:
                start(remote(mid.at[j], mid_in.at[k], pz_s, pz_r, at_z(zup[k])))
        if i == 2:
            arrived(wei.at[pl.ds(0, 7), 0, o_rows], wz_r)
            for d in (2, 1, 3):
                src = wei.at[:, y, o_rows]
                start(remote(src, src, wy_s, wy_r, at_y(ups[d])))
    pl.semaphore_wait(met, 3)
    arrived(mid_in.at[pl.ds(1, 7)], pz_r)
    low = mid[7].astype(F32)
    for k in Z_ORDER:
        low = low + mid_in[k].astype(F32)

    def moments(mean, square, low):
        mean_new = 0.8 * mean + 0.2 * low
        square_new = 0.9 * square + 0.1 * low * low
        return (mean_new, square_new, mean_new / jnp.sqrt(square_new))

    arrived(mq_in, small_sem.at[3])
    arrived(mo_in, small_sem.at[4])
    mq_v[...], sqq_v[...], dir_q = moments(mq_in[0], mq_in[1], low[0:8, 0:qcols])
    mo_v[...], soo_v[...], dir_o = moments(mo_in[0], mo_in[1], low[8:16, :])
    dir_q = jnp.concatenate([dir_q, jnp.zeros((8, 256 - qcols), F32)], axis=1)
    drc[z, y] = jnp.concatenate([dir_q, dir_o], axis=0).astype(BF16)
    sum_q = jnp.sum(dir_q * dir_q, axis=(0, 1), keepdims=True)
    sum_o = jnp.sum(dir_o * dir_o, axis=(0, 1), keepdims=True)
    sums[0] = jnp.concatenate([jnp.broadcast_to(sum_q, (1, 64)), jnp.broadcast_to(sum_o, (1, 64))], axis=1)
    for i, (d, e) in enumerate(SIDE):
        start(remote(sums.at[0], sums_in.at[i], sx_s, sx_r, side(d, e)))
    z_send(d_blk, dz_s, dz_r)
    y_send(d_blk, dy_s, lambda k: dy_r, 0)

    sent(fac.at[core, pl.ds(0, 7), 0], fz_s)
    sent(fac.at[core, pl.ds(0, 6)], fy_s)
    sent(fac.at[core], fd_s)
    sent(wei.at[0, pl.ds(0, 3), q_rows], wb_s)
    sent(wei.at[pl.ds(0, 7), 0, o_rows], wz_s)
    sent(part.at[pl.ds(0, 3)], py_s)
    sent(mid.at[pl.ds(0, 7)], pz_s)
    for g, ks in enumerate(GROUPS):
        arrived(drc.at[pl.ds(0, len(ks)), 0], dz_r.at[g])
        for k in ks:
            y_send(d_blk, dy_s, lambda k: dy_r, k)
    arrived(sums_in.at[pl.ds(0, 31)], sx_r)
    total = sums[0] + jnp.sum(sums_in[0:31], axis=0)
    sums[1] = total

    def sum_copies():
        return [
            remote(sums.at[1], sums_in.at[31 + k], sz_s, sz_r, (zup[k] * NY + y, tp - c))
            for k in FAR_FIRST
            for c in (1, 0)
        ]

    @pl.when(core == 1)
    def _():
        for copy in sum_copies():
            copy.start()

    arrived(drc.at[pl.ds(0, 6)], dy_r)
    every = drc[...].astype(F32).reshape(32, 16, 256)
    pq[...] = dot(factor(0, 16), every[:, 0:8].reshape(256, 256).astype(BF16))
    po[...] = dot(factor(16, 32), every[:, 8:16].reshape(256, 256).astype(BF16))
    arrived(wei.at[:, pl.ds(0, 3), o_rows], wy_r)
    arrived(wei.at[pl.ds(0, 7), :, q_rows], wc_r)
    sent(wei.at[pl.ds(0, 7), :, q_rows], wc_s)
    sent(wei.at[:, pl.ds(0, 3), o_rows], wy_s)
    sent(drc.at[pl.ds(0, 7), 0], dz_s)
    sent(drc.at[pl.ds(0, 6)], dy_s)
    sent(sums_in.at[pl.ds(0, 31)], sx_s)

    @pl.when(core == 1)
    def _():
        sent(sums_in.at[pl.ds(0, 14)], sz_s)

    arrived(sums_in.at[pl.ds(32, 7)], sz_r)
    total = total + jnp.sum(sums_in[32:39], axis=0)
    count = 256.0 * 8 * qcols
    scale_q = lax.rsqrt(total[0:1, 0:1] / count + 0.25)
    scale_o = lax.rsqrt(total[0:1, 64:65] / (256.0 * 8 * 256) + 0.25)

    scales[...] = jnp.concatenate([jnp.broadcast_to(scale_q, (1, 64)), jnp.broadcast_to(scale_o, (1, 64))], axis=1)
    own_q = pq[pl.ds(pl.multiple_of(fs * 16, 16), 16), :][:, 0:qcols] * scale_q
    own_o = po[pl.ds(pl.multiple_of(fs * 32, 32), 32), :] * scale_o
    sq_v[...] = own_q
    so_v[...] = own_o
    nq_v[...] = qw_v[...] - 0.02 * own_q
    no_v[...] = ow_v[...] - 0.02 * own_o


def write_out(
    sq_v, so_v, nq_v, no_v, pq, po, wei, scales, mq_v, sqq_v, mo_v, soo_v,
    step_q, step_o, new_q, new_o, copy_q, copy_o, mean_q, square_q, mean_o, square_o,
    cq, co, sem,
):
    copies = []

    def put(src, dst):
        copies.append(pltpu.make_async_copy(src, dst, sem.at[len(copies)]))
        copies[-1].start()

    for src, dst in (
        (sq_v, step_q), (so_v, step_o), (nq_v, new_q), (no_v, new_o),
        (mq_v, mean_q), (sqq_v, square_q), (mo_v, mean_o), (soo_v, square_o),
    ):
        put(src, dst)
    scale_q, scale_o = scales[0:1, 0:1], scales[0:1, 64:65]

    def weights(levels, rows):
        return wei[levels, :, rows, :].reshape(-1, 256).astype(F32)

    for j in range(4):
        span = pl.ds(256 * j, 256)
        old = weights(slice(2 * j, 2 * j + 2), slice(16, 48))
        co[span, :] = (old - 0.02 * (po[span, :] * scale_o)).astype(BF16)
        put(co.at[span], copy_o.at[span])
        if j == 1:
            old = weights(slice(0, NZ), slice(0, 16))
            cq[...] = (old - 0.02 * (pq[...] * scale_q)).T[0:cq.shape[0], :].astype(BF16)
            put(cq, copy_q)
    for copy in copies:
        copy.wait()


def solution(mesh):
    def on_device(lat, qcot, att, mix, qw, ow, qf, of, qm, qs, om, os_):
        tokens, qcols = lat.shape[0], qw.shape[1]
        inv_root = 1.0 / math.sqrt(tokens * lax.axis_size("fs"))

        def like(a):
            return jax.ShapeDtypeStruct(a.shape, a.dtype)

        def vm(a):
            return pltpu.VMEM(a.shape, a.dtype)

        dma = pltpu.SemaphoreType.DMA
        any_ = pl.BlockSpec(memory_space=pl.ANY)
        outs = (
            like(qw), like(ow), like(qw), like(ow),
            jax.ShapeDtypeStruct((qcols, 512), BF16), jax.ShapeDtypeStruct((1024, 256), BF16),
            like(qm), like(qs), like(om), like(os_),
        )
        kept = [vm(qw), vm(ow), vm(qw), vm(ow)]
        kept += [pltpu.VMEM((512, 256), F32), pltpu.VMEM((1024, 256), F32)]
        kept += [pltpu.VMEM((NZ, NY, 48, 256), BF16), pltpu.VMEM((1, 128), F32)]
        kept += [vm(qm), vm(qs), vm(om), vm(os_)]
        qcot = qcot.T
        held = pl.pallas_call(
            functools.partial(kernel, inv_root),
            out_shape=kept,
            in_specs=[any_] * 12,
            out_specs=[pl.BlockSpec(memory_space=pltpu.VMEM)] * 12,
            scratch_shapes=[
                pltpu.VMEM((tokens, 1792), BF16), vm(qcot), vm(qw), vm(ow),
                pltpu.VMEM((2, 8, qcols), F32), pltpu.VMEM((2, 8, 256), F32),
                pltpu.VMEM((qcols, 512), F32), pltpu.VMEM((256, 1024), F32),
                pltpu.VMEM((qcols, 512), BF16), pltpu.VMEM((256, 1024), BF16),
                pltpu.VMEM((2, NZ, NY, 48, 128), BF16),
                pltpu.VMEM((NY, NZ, 16, 256), BF16), pltpu.VMEM((NY, NZ, 16, 256), BF16),
                pltpu.VMEM((NZ, 16, 256), BF16), pltpu.VMEM((NZ, 16, 256), BF16),
                pltpu.VMEM((NZ, NY, 16, 256), BF16),
                pltpu.VMEM((2, 1, 128), F32), pltpu.VMEM((39, 1, 128), F32),
                dma((CHUNKS, 2)), dma((5,)),
                dma, dma((4,)), dma, dma((5,)), dma, dma,
                dma, dma, dma, dma, dma, dma, dma, dma,
                dma, dma((4,)), dma, dma,
                dma, dma((4,)), dma, dma,
                dma, dma, dma, dma, pltpu.SemaphoreType.REGULAR,
            ],
            compiler_params=pltpu.CompilerParams(
                collective_id=0, has_side_effects=True, vmem_limit_bytes=56 * 1024 * 1024
            ),
        )(lat, qcot, att, mix, qw, ow, qf, of, qm, qs, om, os_)
        results = pl.pallas_call(
            write_out,
            out_shape=outs,
            in_specs=[pl.BlockSpec(memory_space=pltpu.VMEM)] * 12,
            out_specs=[any_] * 10,
            scratch_shapes=[pltpu.VMEM((qcols, 512), BF16), pltpu.VMEM((1024, 256), BF16), dma((13,))],
        )(*[pltpu.with_memory_space_constraint(a, pltpu.VMEM) for a in held])
        return (*results[:4], results[4].T, *results[5:])

    rows, both, whole = P("fs", None), P("fs", "tp"), P(None, "tp")
    return jax.shard_map(
        on_device,
        mesh=mesh,
        in_specs=(rows, both, rows, both, both, both, rows, rows, both, both, both, both),
        out_specs=(both, both, both, both, whole, whole, both, both, both, both),
        check_vma=False,
    )
```
